512 devices in a mesh: sp: 64 (over z, y), tp: 8 (over x, core).
Axes of the slice: x: 4, y: 4, z: 16, core: 2. Of those that a mesh axis runs over, the one named last changes fastest.
Arguments:
- latent: bfloat16 [49152, 2048], P(('sp', 'tp')), may hold values from -6 to 6
- condition: float32 [2048], P('sp'), may hold values from -6 to 6
- context_condition: float32 [2048], P('sp'), may hold values from -6 to 6
- context: bfloat16 [1024, 2048], P('sp'), may hold values from -6 to 6
- norm_gain: float32 [2048], replicated, may hold values from 0.1 to 1.9
- shift_weight: bfloat16 [2048, 2048], P('sp', 'tp'), may hold values from -0.375 to 0.375
- scale_weight: bfloat16 [2048, 2048], P('sp', 'tp'), may hold values from -0.375 to 0.375
- gate_weight: bfloat16 [2048, 2048], P('sp', 'tp'), may hold values from -0.375 to 0.375
- query_weight: bfloat16 [2048, 2048], P(None, 'tp'), may hold values from -2 to 2
- key_matrix: bfloat16 [2048, 1024], P(None, 'tp'), may hold values from -2 to 2
- value_matrix: bfloat16 [2048, 1024], P(None, 'tp'), may hold values from -0.125 to 0.125
- sink_logit_head: float32 [16], P('tp'), may hold values from 6 to 10
- out_weight: bfloat16 [2048, 2048], P('tp'), may hold values from -0.125 to 0.125
Outputs:
- updated: bfloat16 [49152, 2048], P(('sp', 'tp'))
The draws below stay inside these ranges and needn't reach their ends.
All inputs are finite; a program needn't handle non-finite values.
Results may differ from the reference program's by a relative error of at most 0.012.
The reference program's roundings to bfloat16 on the way count: a program that leaves them out, or rounds other values in their place, can miss the bound.
Values may be sent and summed in bfloat16 or wider, within the bound.
No kernel may reach another device: no remote copies, remote signals or barrier semaphores. Data moves between devices by JAX's collectives and lax.ppermute only.
A program may use at most 64 MiB of HBM per device.

```python
import jax
import jax.numpy as jnp
from jax import lax

MODEL_DIM = 2048
QUERY_HEADS = 16
KEY_VALUE_HEADS = 8
HEAD_DIM = 128
WINDOW_REACH = 128
GRID_W = 64
CTX = 1024
TOKENS = 49152
N_TP = 8


def query_shared_group(key):
    return jax.random.normal(jax.random.fold_in(key, 101), (MODEL_DIM, QUERY_HEADS * HEAD_DIM), jnp.float32) * MODEL_DIM ** (-0.5)


def draw_query_weight(key, part):
    return query_shared_group(key).astype(jnp.bfloat16)


def draw_key_matrix(key, part):
    sampled_weights = jax.random.normal(jax.random.fold_in(key, 202), (MODEL_DIM, KEY_VALUE_HEADS * HEAD_DIM), jnp.float32) * MODEL_DIM ** (-0.5)
    return sampled_weights.astype(jnp.bfloat16)


def raised(drawn, stream_key, source, target, shards_of, factor):
    owner, partner = [(jnp.arange(drawn.shape[dim]) // (drawn.shape[dim] // shards_of)).reshape([-1 if axis == dim else 1 for axis in range(drawn.ndim)]) for dim in (source, target)]
    chosen = jax.random.permutation(stream_key, shards_of)[partner]
    strong = (owner == chosen) | (owner == (partner + shards_of // 2) % shards_of)
    return jnp.where(strong, factor * drawn, drawn)


def level_of(stream_key, dims, cuts, low, top_value):
    def one(axis_at, parts):
        steps = jax.random.uniform(jax.random.fold_in(jax.random.fold_in(stream_key, 6), axis_at), (parts,), jnp.float32, low / len(cuts), top_value / len(cuts))
        return jnp.repeat(jnp.exp(steps), dims[axis_at] // parts).reshape((-1,) + (1,) * (len(dims) - axis_at - 1))

    gain = one(*cuts[0])
    for cut in cuts[1:]:
        gain = gain * one(*cut)
    return gain


def normal_values(key, dims, spread, most, cuts=(), kind=jnp.bfloat16):
    drawn = spread * jax.random.normal(key, dims, jnp.float32)
    if cuts:
        drawn = drawn * level_of(key, dims, cuts, -0.22, 0.18)
    return jnp.clip(drawn, -most, most).astype(kind)


def heavy_noise(stream_key, extent, scale, most, cuts, heavy, kind=jnp.bfloat16):
    values = scale * jax.random.normal(stream_key, extent, jnp.float32)
    if cuts:
        values = values * level_of(stream_key, extent, cuts, -0.22, 0.18)
    return jnp.clip(raised(values, jax.random.fold_in(stream_key, 3), *heavy), -most, most).astype(kind)


def setup_inputs(seed: int = 0) -> dict:
    key_list = jax.random.split(jax.random.key(seed), 14)
    latent = normal_values(key_list[0], (TOKENS, MODEL_DIM), 1.0, 6.0, ((0, 512),))
    condition = normal_values(key_list[1], (MODEL_DIM,), 1.0, 6.0, ((0, 64),), jnp.float32)
    context_condition = normal_values(key_list[2], (MODEL_DIM,), 1.0, 6.0, ((0, 64),), jnp.float32)
    context = normal_values(key_list[3], (CTX, MODEL_DIM), 1.0, 6.0, ((0, 64),))
    norm_gain = jnp.clip(1.0 + 0.18 * jax.random.normal(key_list[4], (MODEL_DIM,), jnp.float32), 0.1, 1.9)
    shift_weight = heavy_noise(key_list[5], (MODEL_DIM, MODEL_DIM), MODEL_DIM ** -0.5, 0.375, ((0, 64), (1, 8)), (0, 1, 64, 4.0))
    scale_weight = heavy_noise(key_list[6], (MODEL_DIM, MODEL_DIM), MODEL_DIM ** -0.5, 0.375, ((0, 64), (1, 8)), (0, 1, 64, 4.0))
    gate_weight = heavy_noise(key_list[7], (MODEL_DIM, MODEL_DIM), MODEL_DIM ** -0.5, 0.375, ((0, 64), (1, 8)), (0, 1, 64, 4.0))
    query_weight = draw_query_weight(jax.random.fold_in(key_list[13], 71), 0)
    key_matrix = draw_key_matrix(jax.random.fold_in(key_list[13], 71), 0)
    value_matrix = normal_values(key_list[10], (MODEL_DIM, KEY_VALUE_HEADS * HEAD_DIM), MODEL_DIM ** -0.5, 0.125, ((1, 8),))
    sink_logit_head = jnp.clip(6.0 + 4.0 * jax.random.uniform(key_list[11], (QUERY_HEADS,), jnp.float32) ** level_of(key_list[11], (QUERY_HEADS,), ((0, 8),), -0.2, 0.2), 6.0, 10.0)
    out_weight = normal_values(key_list[12], (QUERY_HEADS * HEAD_DIM, MODEL_DIM), (QUERY_HEADS * HEAD_DIM) ** -0.5, 0.125, ((0, 8),))
    return {"latent": latent, "condition": condition, "context_condition": context_condition, "context": context, "norm_gain": norm_gain, "shift_weight": shift_weight, "scale_weight": scale_weight, "gate_weight": gate_weight, "query_weight": query_weight, "key_matrix": key_matrix, "value_matrix": value_matrix, "sink_logit_head": sink_logit_head, "out_weight": out_weight}


NORM_EPS = 1e-05
MASKED_SCORE = -1e+30

def rotate(vectors, position):
    quarter = HEAD_DIM // 4
    grid_row = (position // GRID_W).astype(jnp.float32)
    grid_col = (position % GRID_W).astype(jnp.float32)
    inv_freq = 10000.0 ** (-jnp.arange(0, HEAD_DIM // 2, 2, dtype=jnp.float32) / (HEAD_DIM // 2))
    angles = jnp.concatenate([grid_row[:, None] * inv_freq, grid_col[:, None] * inv_freq], axis=-1)
    cosine_table = jnp.cos(angles).reshape(-1, 1, 2, quarter)
    sine_table = jnp.sin(angles).reshape(-1, 1, 2, quarter)
    pieces = vectors.reshape(vectors.shape[0], vectors.shape[1], 2, 2, quarter)
    first_half = pieces[..., 0, :]
    second_half = pieces[..., 1, :]
    turned = jnp.stack([first_half * cosine_table - second_half * sine_table, first_half * sine_table + second_half * cosine_table], axis=-2)
    return turned.reshape(vectors.shape)

def modulation(vector, weight):
    active = jax.nn.silu(vector).astype(jnp.bfloat16)
    return jnp.dot(active[None, :], weight, preferred_element_type=jnp.float32)[0]

def modulated_norm(rows_in, norm_gain, shift, scale):
    floats = rows_in.astype(jnp.float32)
    normed = floats * lax.rsqrt(lax.optimization_barrier(jnp.mean(floats * floats, axis=-1, keepdims=True)) + NORM_EPS) * norm_gain
    return (normed * (1.0 + scale) + shift).astype(jnp.bfloat16)

def attend(queries, joined_keys, joined_values, context_key_rows, context_value_rows, sink_logit_head):
    latent_token_count = queries.shape[0]
    blocks = latent_token_count // WINDOW_REACH
    queries_per_group = QUERY_HEADS // KEY_VALUE_HEADS
    padding = ((WINDOW_REACH, WINDOW_REACH), (0, 0), (0, 0))
    keys_pad = jnp.pad(joined_keys, padding)
    values_pad = jnp.pad(joined_values, padding)
    ctx_key_f = context_key_rows.astype(jnp.float32)
    ctx_value_f = context_value_rows.astype(jnp.float32)
    factor = HEAD_DIM ** (-0.5)
    sink_logit_rows = sink_logit_head.reshape(KEY_VALUE_HEADS, queries_per_group, 1, 1)

    def one_block(block_index):
        begin_row = block_index * WINDOW_REACH
        query_row_block = lax.dynamic_slice_in_dim(queries, begin_row, WINDOW_REACH, 0)
        query_row_block = query_row_block.reshape(WINDOW_REACH, KEY_VALUE_HEADS, queries_per_group, HEAD_DIM).astype(jnp.float32)
        band_keys = lax.dynamic_slice_in_dim(keys_pad, begin_row, 3 * WINDOW_REACH, 0).astype(jnp.float32)
        band_values = lax.dynamic_slice_in_dim(values_pad, begin_row, 3 * WINDOW_REACH, 0).astype(jnp.float32)
        band_scores = jnp.einsum('qhgd,khd->hgqk', query_row_block, band_keys) * factor
        query_pos = begin_row + jnp.arange(WINDOW_REACH, dtype=jnp.int32)[:, None]
        key_pos = begin_row - WINDOW_REACH + jnp.arange(3 * WINDOW_REACH, dtype=jnp.int32)[None, :]
        allowed = (jnp.abs(key_pos - query_pos) <= WINDOW_REACH) & (key_pos >= 0) & (key_pos < latent_token_count)
        band_scores = jnp.where(allowed[None, None], band_scores, MASKED_SCORE)
        ctx_scores = jnp.einsum('qhgd,chd->hgqc', query_row_block, ctx_key_f) * factor
        maxima = jnp.maximum(jnp.maximum(lax.optimization_barrier(jnp.max(band_scores, axis=-1, keepdims=True)), lax.optimization_barrier(jnp.max(ctx_scores, axis=-1, keepdims=True))), sink_logit_rows)
        band_exp = jnp.exp(band_scores - maxima)
        ctx_exp = jnp.exp(ctx_scores - maxima)
        denominator = lax.optimization_barrier(jnp.sum(band_exp, axis=-1, keepdims=True)) + lax.optimization_barrier(jnp.sum(ctx_exp, axis=-1, keepdims=True)) + jnp.exp(sink_logit_rows - maxima)
        band_weights = (band_exp / denominator).astype(jnp.bfloat16).astype(jnp.float32)
        ctx_weights = (ctx_exp / denominator).astype(jnp.bfloat16).astype(jnp.float32)
        summed = jnp.einsum('hgqk,khd->qhgd', band_weights, band_values) + jnp.einsum('hgqc,chd->qhgd', ctx_weights, ctx_value_f)
        return summed.astype(jnp.bfloat16).reshape(WINDOW_REACH, QUERY_HEADS * HEAD_DIM)
    blocks_out = lax.map(one_block, jnp.arange(blocks, dtype=jnp.int32))
    return blocks_out.reshape(latent_token_count, QUERY_HEADS * HEAD_DIM)

def reference(latent, condition, context_condition, context, norm_gain, shift_weight, scale_weight, gate_weight, query_weight, key_matrix, value_matrix, sink_logit_head, out_weight):
    shift = modulation(condition, shift_weight)
    scale = modulation(condition, scale_weight)
    gate = modulation(condition, gate_weight)
    ctx_shift = modulation(context_condition, shift_weight)
    ctx_scale = modulation(context_condition, scale_weight)
    hidden_state = modulated_norm(latent, norm_gain, shift, scale)
    ctx_hidden = modulated_norm(context, norm_gain, ctx_shift, ctx_scale)
    latent_token_count = latent.shape[0]
    position = jnp.arange(latent_token_count, dtype=jnp.int32)
    queries = jnp.dot(hidden_state, query_weight, preferred_element_type=jnp.float32).reshape(latent_token_count, QUERY_HEADS, HEAD_DIM)
    queries = rotate(queries, position).astype(jnp.bfloat16)
    joined_keys = jnp.dot(hidden_state, key_matrix, preferred_element_type=jnp.float32).reshape(latent_token_count, KEY_VALUE_HEADS, HEAD_DIM)
    joined_keys = rotate(joined_keys, position).astype(jnp.bfloat16)
    joined_values = jnp.dot(hidden_state, value_matrix, preferred_element_type=jnp.float32).astype(jnp.bfloat16)
    joined_values = joined_values.reshape(latent_token_count, KEY_VALUE_HEADS, HEAD_DIM)
    context_key_rows = jnp.dot(ctx_hidden, key_matrix, preferred_element_type=jnp.float32).astype(jnp.bfloat16)
    context_value_rows = jnp.dot(ctx_hidden, value_matrix, preferred_element_type=jnp.float32).astype(jnp.bfloat16)
    context_key_rows = context_key_rows.reshape(-1, KEY_VALUE_HEADS, HEAD_DIM)
    context_value_rows = context_value_rows.reshape(-1, KEY_VALUE_HEADS, HEAD_DIM)
    attended = attend(queries, joined_keys, joined_values, context_key_rows, context_value_rows, sink_logit_head)
    group_width = QUERY_HEADS * HEAD_DIM // N_TP
    mixed_sum = jnp.zeros((latent_token_count, latent.shape[1]), jnp.float32)
    for member in range(N_TP):
        partial_value = jnp.dot(attended[:, member * group_width:(member + 1) * group_width], out_weight[member * group_width:(member + 1) * group_width], preferred_element_type=jnp.float32)
        rounded = lax.optimization_barrier(partial_value.astype(jnp.bfloat16))
        mixed_sum = mixed_sum + rounded.astype(jnp.float32)
    return (latent.astype(jnp.float32) + gate * mixed_sum).astype(jnp.bfloat16)
```

```python
import jax
import jax.numpy as jnp
from jax import lax
from jax.sharding import Mesh
from jax.sharding import PartitionSpec as P

QUERY_HEADS = 16
KEY_VALUE_HEADS = 8
HEAD_DIM = 128
WINDOW_REACH = 128
GRID_W = 64
SP = ("z", "y")
TP = ("x", "c")
PLANE = ("y", "x", "c")
ALL = ("z", "y", "x", "c")

NORM_EPS = 1e-05
MASKED_SCORE = -1e30


def sent_to_all(x, axis):
    peers = lax.axis_size(axis)
    return lax.all_to_all(jnp.broadcast_to(x[None], (peers, *x.shape)), axis, 0, 0, tiled=True)


def padded_2(block, axis, width):
    count = lax.axis_size(axis)
    forward = [(i, i + 1) for i in range(count - 1)]
    backward = [(target, source) for source, target in forward]
    low = lax.ppermute(block[block.shape[0] - width :], axis, forward)
    high = lax.ppermute(block[:width], axis, backward)
    return jnp.concatenate([low, block, high], axis=0)


def rotate(vectors, position):
    quarter = HEAD_DIM // 4
    grid_row = (position // GRID_W).astype(jnp.float32)
    grid_col = (position % GRID_W).astype(jnp.float32)
    inv_freq = 10000.0 ** (-jnp.arange(0, HEAD_DIM // 2, 2, dtype=jnp.float32) / (HEAD_DIM // 2))
    angles = jnp.concatenate([grid_row[:, None] * inv_freq, grid_col[:, None] * inv_freq], axis=-1)
    cosine_table = jnp.cos(angles).reshape(-1, 1, 2, quarter)
    sine_table = jnp.sin(angles).reshape(-1, 1, 2, quarter)
    pieces = vectors.reshape(vectors.shape[0], vectors.shape[1], 2, 2, quarter)
    first_half = pieces[..., 0, :]
    second_half = pieces[..., 1, :]
    turned = jnp.stack(
        [
            first_half * cosine_table - second_half * sine_table,
            first_half * sine_table + second_half * cosine_table,
        ],
        axis=-2,
    )
    return turned.reshape(vectors.shape)


def modulated_norm(rows_in, norm_gain, shift, scale):
    floats = rows_in.astype(jnp.float32)
    normed = (
        floats * lax.rsqrt(jnp.mean(floats * floats, axis=-1, keepdims=True) + NORM_EPS) * norm_gain
    )
    return (normed * (1.0 + scale) + shift).astype(jnp.bfloat16)


def shards(
    latent,
    condition,
    context_condition,
    context,
    norm_gain,
    shift_weight,
    scale_weight,
    gate_weight,
    query_weight,
    key_matrix,
    value_matrix,
    sink_logit_head,
    out_weight,
):
    nz, ny, nx, nc = (lax.axis_size(a) for a in ALL)
    rows, width = latent.shape
    group_rows = rows * nx * nc
    offset = lax.axis_index(SP) * group_rows
    total_rows = group_rows * nz * ny
    latent_x = sent_to_all(latent, "x")
    active = jax.nn.silu(jnp.stack([condition, context_condition])).astype(jnp.bfloat16)
    shift_part = jnp.dot(active, shift_weight, preferred_element_type=jnp.float32)
    scale_part = jnp.dot(active, scale_weight, preferred_element_type=jnp.float32)
    gate_part = jnp.dot(active[:1], gate_weight, preferred_element_type=jnp.float32)
    parts = jnp.concatenate([shift_part, scale_part, gate_part], axis=0)
    columns = parts.shape[1]
    coarse = parts.astype(jnp.bfloat16)
    fine = (parts - coarse.astype(jnp.float32)).astype(jnp.bfloat16)
    share = context.shape[0] // (nx * nc)
    mine = lax.dynamic_slice_in_dim(context, lax.axis_index(TP) * share, share, 0)
    mine = mine.reshape(-1, columns)
    sent = jnp.concatenate([mine, coarse, fine], axis=0)
    got = sent_to_all(sent, "z")
    ctx_z = got[:, : mine.shape[0]].reshape(nz * share, width)
    halves = got[:, mine.shape[0] :].astype(jnp.float32)
    z_sum = jnp.sum(halves[:, :5] + halves[:, 5:], axis=0)
    planes = sent_to_all(z_sum.reshape(1, -1), PLANE)
    ctx_x = sent_to_all(ctx_z, "x")
    latent_all = sent_to_all(latent_x, "c").reshape(nc, nx, rows, width)
    ctx_all = sent_to_all(ctx_x.reshape(-1, width), "c").reshape(-1, width)
    mods = jnp.sum(planes.reshape(ny, nx * nc, 5, columns), axis=0)
    mods = jnp.moveaxis(mods, 0, 1).reshape(5, width)
    shift, ctx_shift, scale, ctx_scale, gate = (mods[i] for i in range(5))
    ctx_hidden = modulated_norm(ctx_all, norm_gain, ctx_shift, ctx_scale)
    ctx_pairs = sent_to_all(
        jnp.concatenate(
            [
                jnp.dot(ctx_hidden, key_matrix, preferred_element_type=jnp.float32),
                jnp.dot(ctx_hidden, value_matrix, preferred_element_type=jnp.float32),
            ],
            axis=1,
        ).astype(jnp.bfloat16),
        "y",
    )
    ctx_pairs = ctx_pairs.reshape(-1, ctx_pairs.shape[-1])
    query_width = query_weight.shape[1]
    pair_width = key_matrix.shape[1]
    block_rows = modulated_norm(latent_all, norm_gain, shift, scale).reshape(group_rows, width)
    position = (
        offset
        + jnp.arange(nc, dtype=jnp.int32)[:, None, None] * rows
        + jnp.arange(nx, dtype=jnp.int32)[None, :, None] * (rows * nc)
        + jnp.arange(rows, dtype=jnp.int32)[None, None, :]
    ).reshape(-1)
    query_rows = jnp.dot(block_rows, query_weight, preferred_element_type=jnp.float32)
    query_rows = rotate(query_rows.reshape(group_rows, -1, HEAD_DIM), position)
    key_rows = jnp.dot(block_rows, key_matrix, preferred_element_type=jnp.float32)
    key_rows = rotate(key_rows.reshape(group_rows, -1, HEAD_DIM), position)
    value_rows = jnp.dot(block_rows, value_matrix, preferred_element_type=jnp.float32)
    projected = jnp.concatenate(
        [
            query_rows.reshape(group_rows, query_width),
            key_rows.reshape(group_rows, pair_width),
            value_rows,
        ],
        axis=1,
    ).astype(jnp.bfloat16)
    projected = jnp.swapaxes(projected.reshape(nc, nx, rows, -1), 0, 1).reshape(group_rows, -1)
    padded = padded_2(projected[:, query_width:], SP, WINDOW_REACH)
    blocks = group_rows // WINDOW_REACH
    kv_local = pair_width // HEAD_DIM
    queries_per_group = QUERY_HEADS // KEY_VALUE_HEADS
    query_blocks = projected[:, :query_width].reshape(
        blocks, WINDOW_REACH, kv_local, queries_per_group, HEAD_DIM
    )
    key_pad = padded[:, :pair_width].reshape(blocks + 2, WINDOW_REACH, kv_local, HEAD_DIM)
    value_pad = padded[:, pair_width:].reshape(blocks + 2, WINDOW_REACH, kv_local, HEAD_DIM)
    band_keys = jnp.concatenate([key_pad[:-2], key_pad[1:-1], key_pad[2:]], axis=1)
    band_values = jnp.concatenate([value_pad[:-2], value_pad[1:-1], value_pad[2:]], axis=1)
    context_key_rows = ctx_pairs[:, :pair_width].reshape(-1, kv_local, HEAD_DIM)
    context_value_rows = ctx_pairs[:, pair_width:].reshape(-1, kv_local, HEAD_DIM)
    factor = HEAD_DIM ** (-0.5)
    band_scores = (
        jnp.einsum("nqhgd,nkhd->nhgqk", query_blocks, band_keys, preferred_element_type=jnp.float32)
        * factor
    )
    block_ids = jnp.arange(blocks, dtype=jnp.int32)[:, None, None]
    query_pos = (
        offset + block_ids * WINDOW_REACH + jnp.arange(WINDOW_REACH, dtype=jnp.int32)[None, :, None]
    )
    key_pos = (
        offset
        + (block_ids - 1) * WINDOW_REACH
        + jnp.arange(3 * WINDOW_REACH, dtype=jnp.int32)[None, None, :]
    )
    allowed = (
        (jnp.abs(key_pos - query_pos) <= WINDOW_REACH) & (key_pos >= 0) & (key_pos < total_rows)
    )
    band_scores = jnp.where(allowed[:, None, None], band_scores, MASKED_SCORE)
    ctx_scores = (
        jnp.einsum(
            "nqhgd,chd->nhgqc", query_blocks, context_key_rows, preferred_element_type=jnp.float32
        )
        * factor
    )
    sink_logit_rows = sink_logit_head.reshape(1, kv_local, queries_per_group, 1, 1)
    maxima = jnp.maximum(
        jnp.maximum(
            jnp.max(band_scores, axis=-1, keepdims=True),
            jnp.max(ctx_scores, axis=-1, keepdims=True),
        ),
        sink_logit_rows,
    )
    band_exp = jnp.exp(band_scores - maxima)
    ctx_exp = jnp.exp(ctx_scores - maxima)
    denominator = (
        jnp.sum(band_exp, axis=-1, keepdims=True)
        + jnp.sum(ctx_exp, axis=-1, keepdims=True)
        + jnp.exp(sink_logit_rows - maxima)
    )
    band_weights = (band_exp / denominator).astype(jnp.bfloat16)
    ctx_weights = (ctx_exp / denominator).astype(jnp.bfloat16)
    attended = jnp.einsum(
        "nhgqk,nkhd->nqhgd", band_weights, band_values, preferred_element_type=jnp.float32
    ) + jnp.einsum(
        "nhgqc,chd->nqhgd", ctx_weights, context_value_rows, preferred_element_type=jnp.float32
    )
    attended = attended.astype(jnp.bfloat16).reshape(nx, nc, rows, query_width)
    attended = jnp.swapaxes(attended, 0, 1).reshape(group_rows, query_width)
    partial = jnp.dot(attended, out_weight, preferred_element_type=jnp.float32)
    partial = partial.astype(jnp.bfloat16).reshape(nc, nx * rows, width)
    pair = lax.all_to_all(partial, "c", 0, 0, tiled=True)
    pair = jnp.sum(pair.astype(jnp.float32), axis=0).astype(jnp.bfloat16)
    mixed = lax.all_to_all(pair.reshape(nx, rows, width), "x", 0, 0, tiled=True)
    mixed = jnp.sum(mixed.astype(jnp.float32), axis=0)
    return (latent.astype(jnp.float32) + gate * mixed).astype(jnp.bfloat16)


def solution(mesh):
    torus = Mesh(mesh.devices.reshape(16, 4, 4, 2), ALL)
    return jax.shard_map(
        shards,
        mesh=torus,
        in_specs=(
            P(ALL, None),
            P(SP),
            P(SP),
            P(SP, None),
            P(),
            P(SP, TP),
            P(SP, TP),
            P(SP, TP),
            P(None, TP),
            P(None, TP),
            P(None, TP),
            P(TP),
            P(TP, None),
        ),
        out_specs=P(ALL, None),
        check_vma=False,
    )
```

```python
import jax
import jax.numpy as jnp
from jax import lax
from jax.experimental import pallas as pl
from jax.experimental.pallas import tpu as pltpu
from jax.sharding import Mesh
from jax.sharding import PartitionSpec as P

HEAD_DIM = 128
WINDOW_REACH = 128
GRID_W = 64
SP = ("z", "y")
TP = ("x", "c")
PLANE = ("y", "x", "c")
ALL = ("z", "y", "x", "c")
NORM_EPS = 1e-05
MASKED_SCORE = -1e30
LOG2_E = 1.4426950408889634
CHUNK = 16


VMEM = pl.BlockSpec(memory_space=pltpu.VMEM)
SMEM = pl.BlockSpec(memory_space=pltpu.SMEM)
F32 = jnp.float32
BF16 = jnp.bfloat16


def shape_of(shape, dtype):
    return jax.ShapeDtypeStruct(shape, dtype)


def copies(x, axis):
    return jnp.broadcast_to(x[None], (lax.axis_size(axis), *x.shape))


def exchanged(blocks, axis):
    return lax.all_to_all(blocks, axis, 0, 0, tiled=True)


def dot(a, b):
    return jnp.dot(a, b, preferred_element_type=F32)


def row_vector(planes_ref, index, columns):
    count = planes_ref.shape[0] // 4
    cut = pl.ds(index * columns, columns)
    pieces = []
    for t in range(count):
        piece = planes_ref[t, :, cut]
        for y in range(1, 4):
            piece = piece + planes_ref[y * count + t, :, cut]
        pieces.append(piece)
    return jnp.concatenate(pieces, axis=1)


def parts_kernel(
    member_ref, cond_ref, ctx_cond_ref, shift_ref, scale_ref, gate_ref, ctx_ref, out_ref
):
    def active(ref):
        v = ref[...]
        return (v / (1.0 + jnp.exp(-v))).astype(BF16)

    both = jnp.concatenate([active(cond_ref), active(ctx_cond_ref)], axis=0)
    both = jnp.concatenate([both, jnp.zeros((14, both.shape[1]), BF16)], axis=0)
    shift = dot(both, shift_ref[...])
    scale = dot(both, scale_ref[...])
    gate = dot(both, gate_ref[...])
    width = ctx_ref.shape[1]
    blank = jnp.zeros((1, width - 5 * shift.shape[1]), F32)
    row = jnp.concatenate(
        [shift[0:1], shift[1:2], scale[0:1], scale[1:2], gate[0:1], blank], axis=1
    )
    coarse = row.astype(BF16).astype(F32)
    ctx = ctx_ref[...].astype(F32)
    at = lax.broadcasted_iota(jnp.int32, (ctx.shape[0], 1), 0)
    picked = [
        jnp.sum(jnp.where(at == 2 * member_ref[0] + i, ctx, 0.0), axis=0, keepdims=True)
        for i in range(2)
    ]
    rows = jnp.concatenate(picked + [coarse, row - coarse], axis=0).astype(BF16)
    for i in range(out_ref.shape[0]):
        out_ref[i] = rows


def normed_rows(ref, x, start, multiplier, shift):
    rows = ref[x, pl.ds(start, CHUNK), :].astype(F32)
    mean = jnp.mean(rows * rows, axis=-1, keepdims=True)
    return (rows * lax.rsqrt(mean + NORM_EPS) * multiplier + shift).astype(BF16)


def turned(u, cosine, sine):
    lane = lax.broadcasted_iota(jnp.int32, u.shape, 1)
    first = (lane % 64) < 32
    swapped = jnp.where(first, pltpu.roll(u, 96, 1), pltpu.roll(u, 32, 1))
    return u * cosine + swapped * sine


def qkv_kernel(
    base_ref, own_ref, other_ref, planes_ref, gain_ref, wq_ref, wkv_ref, cos_ref, sin_ref,
    q_ref, kv_ref, hidden_ref,
):
    columns = wq_ref.shape[1]
    shift = row_vector(planes_ref, 0, columns)
    multiplier = gain_ref[...] * (1.0 + row_vector(planes_ref, 2, columns))
    count, rows, _ = own_ref.shape
    steps = rows // CHUNK

    def step(i, carry):
        x = i // steps
        start = pl.multiple_of((i % steps) * CHUNK, CHUNK)
        at = pl.multiple_of(base_ref[x] + start, CHUNK)
        hidden_ref[pl.ds(at, CHUNK), :] = normed_rows(own_ref, x, start, multiplier, shift)
        at = pl.multiple_of(base_ref[count + x] + start, CHUNK)
        hidden_ref[pl.ds(at, CHUNK), :] = normed_rows(other_ref, x, start, multiplier, shift)
        return carry

    lax.fori_loop(0, count * steps, step, 0)
    block = 384
    for at in range(0, hidden_ref.shape[0], block):
        cut = slice(at, at + block)
        hidden = hidden_ref[cut, :]
        cosine, sine = cos_ref[cut, :], sin_ref[cut, :]
        queries = dot(hidden, wq_ref[...])
        q_ref[cut, :HEAD_DIM] = turned(queries[:, :HEAD_DIM], cosine, sine).astype(BF16)
        q_ref[cut, HEAD_DIM:] = turned(queries[:, HEAD_DIM:], cosine, sine).astype(BF16)
        pairs = dot(hidden, wkv_ref[...])
        kv_ref[cut, :HEAD_DIM] = turned(pairs[:, :HEAD_DIM], cosine, sine).astype(BF16)
        kv_ref[cut, HEAD_DIM:] = pairs[:, HEAD_DIM:].astype(BF16)


def context_kernel(own_ref, other_ref, planes_ref, gain_ref, wkv_ref, out_ref, hidden_ref):
    columns = wkv_ref.shape[1]
    shift = row_vector(planes_ref, 1, columns)
    multiplier = gain_ref[...] * (1.0 + row_vector(planes_ref, 3, columns))
    count, rows, _ = own_ref.shape
    steps = rows // CHUNK
    half = count * rows

    def step(i, carry):
        x = i // steps
        start = pl.multiple_of((i % steps) * CHUNK, CHUNK)
        at = pl.multiple_of(x * rows + start, CHUNK)
        hidden_ref[pl.ds(at, CHUNK), :] = normed_rows(own_ref, x, start, multiplier, shift)
        at = pl.multiple_of(half + x * rows + start, CHUNK)
        hidden_ref[pl.ds(at, CHUNK), :] = normed_rows(other_ref, x, start, multiplier, shift)
        return carry

    lax.fori_loop(0, count * steps, step, 0)
    pairs = dot(hidden_ref[...], wkv_ref[...]).astype(BF16)
    for y in range(out_ref.shape[0]):
        out_ref[y] = pairs


def attention_kernel(
    place_ref, sink_ref, q_ref, low_ref, kv_ref, high_ref, ctx_ref, weight_ref,
    keep_ref, send_ref, padded_ref, attended_ref, gathered_ref,
):
    reach = WINDOW_REACH
    total = kv_ref.shape[0]
    core, first, last = place_ref[0], place_ref[1], place_ref[2]
    padded_ref[:reach, :] = low_ref[...]
    padded_ref[reach : reach + total, :] = kv_ref[...]
    padded_ref[reach + total :, :] = high_ref[...]
    ctx = ctx_ref[...].reshape(-1, 2 * HEAD_DIM)
    ctx_keys, ctx_values = ctx[:, :HEAD_DIM], ctx[:, HEAD_DIM:]
    factor = HEAD_DIM ** (-0.5) * LOG2_E
    row = lax.broadcasted_iota(jnp.int32, (2 * reach, 1), 0)
    sink = jnp.where(row < reach, sink_ref[0], sink_ref[1]) * LOG2_E
    position = lax.broadcasted_iota(jnp.int32, (2 * reach, 3 * reach), 0) % reach
    column = lax.broadcasted_iota(jnp.int32, (2 * reach, 3 * reach), 1)
    band = (column >= position) & (column <= position + 2 * reach)
    blocks = total // reach
    contract = (((1,), (1,)), ((), ()))

    def step(b, carry):
        at = pl.multiple_of(b * reach, reach)
        both = q_ref[pl.ds(at, reach), :]
        queries = jnp.concatenate([both[:, :HEAD_DIM], both[:, HEAD_DIM:]], axis=0)
        keys = padded_ref[pl.ds(at, 3 * reach), :HEAD_DIM]
        values = padded_ref[pl.ds(at, 3 * reach), HEAD_DIM:]
        lowest = jnp.where(b == 0, first * reach, 0)
        highest = jnp.where(b == blocks - 1, (3 - last) * reach, 3 * reach)
        allowed = band & (column >= lowest) & (column < highest)
        near = lax.dot_general(queries, keys, contract, preferred_element_type=F32) * factor
        near = jnp.where(allowed, near, MASKED_SCORE)
        far = lax.dot_general(queries, ctx_keys, contract, preferred_element_type=F32) * factor
        top = jnp.maximum(
            jnp.max(near, axis=-1, keepdims=True), jnp.max(far, axis=-1, keepdims=True)
        )
        top = jnp.maximum(top, sink)
        near = jnp.exp2(near - top)
        far = jnp.exp2(far - top)
        share = (
            jnp.sum(near, axis=-1, keepdims=True)
            + jnp.sum(far, axis=-1, keepdims=True)
            + jnp.exp2(sink - top)
        )
        mixed = dot(near.astype(BF16), values) + dot(far.astype(BF16), ctx_values)
        mixed = (mixed / share).astype(BF16)
        attended_ref[pl.ds(at, reach), :HEAD_DIM] = mixed[:reach]
        attended_ref[pl.ds(at, reach), HEAD_DIM:] = mixed[reach:]
        return carry

    lax.fori_loop(0, blocks, step, 0)
    rows = keep_ref.shape[0] // 4
    for x in range(4):
        mine = pl.multiple_of((2 * x + core) * rows, CHUNK)
        theirs = pl.multiple_of((2 * x + 1 - core) * rows, CHUNK)
        keep_ref[x * rows : (x + 1) * rows, :] = attended_ref[pl.ds(mine, rows), :]
        gathered_ref[x * rows : (x + 1) * rows, :] = attended_ref[pl.ds(theirs, rows), :]
    width = 512
    for n in range(0, send_ref.shape[1], width):
        send_ref[:, n : n + width] = dot(
            gathered_ref[...], weight_ref[:, n : n + width]
        ).astype(BF16)


def pair_kernel(keep_ref, weight_ref, got_ref, out_ref):
    width = 512
    count, rows, _ = out_ref.shape
    for n in range(0, got_ref.shape[1], width):
        cut = slice(n, n + width)
        both = dot(keep_ref[...], weight_ref[:, cut]) + got_ref[:, cut].astype(F32)
        out_ref[:, :, cut] = both.astype(BF16).reshape(count, rows, width)


def final_kernel(latent_ref, mixed_ref, planes_ref, out_ref):
    count = mixed_ref.shape[0]
    columns = planes_ref.shape[2] // 5
    gate = row_vector(planes_ref, 4, columns)

    def step(i, carry):
        cut = pl.ds(pl.multiple_of(i * CHUNK, CHUNK), CHUNK)
        mixed = mixed_ref[0, cut, :].astype(F32)
        for x in range(1, count):
            mixed = mixed + mixed_ref[x, cut, :].astype(F32)
        out_ref[cut, :] = (latent_ref[cut, :].astype(F32) + gate * mixed).astype(BF16)
        return carry

    lax.fori_loop(0, latent_ref.shape[0] // CHUNK, step, 0)


SHIFTS = (0, 1, 3, 2)


def from_all_x(block):
    got = [block]
    for shift in SHIFTS[1:]:
        got.append(lax.ppermute(block, "x", [(i, (i + shift) % 4) for i in range(4)]))
    return jnp.stack(got)


def swapped(x):
    return lax.ppermute(x, "c", [(0, 1), (1, 0)])


def tables(position):
    inv_freq = 10000.0 ** (-jnp.arange(0, HEAD_DIM // 2, 2, dtype=F32) / (HEAD_DIM // 2))
    by_row = (position // GRID_W).astype(F32)[:, None] * inv_freq
    by_col = (position % GRID_W).astype(F32)[:, None] * inv_freq
    angles = jnp.concatenate([by_row, by_row, by_col, by_col], axis=1)
    sign = jnp.where((jnp.arange(HEAD_DIM) % 64) < 32, -1.0, 1.0).astype(F32)
    return jnp.cos(angles), jnp.sin(angles) * sign


def shards(
    latent,
    condition,
    context_condition,
    context,
    norm_gain,
    shift_weight,
    scale_weight,
    gate_weight,
    query_weight,
    key_matrix,
    value_matrix,
    sink_logit_head,
    out_weight,
):
    nz, ny, nx, nc = (lax.axis_size(a) for a in ALL)
    rows, width = latent.shape
    group_rows = rows * nx * nc
    columns = shift_weight.shape[1]
    place = lax.axis_index(SP)
    core = lax.axis_index("c").astype(jnp.int32)
    gain = norm_gain.reshape(1, width)
    member = lax.axis_index(TP).astype(jnp.int32)
    share = context.shape[0] // (nx * nc)
    parts = pl.pallas_call(
        parts_kernel,
        out_shape=shape_of((nz, share + 2, width), BF16),
        in_specs=[SMEM] + [VMEM] * 6,
        out_specs=VMEM,
        name="parts",
    )(
        member[None],
        condition.reshape(1, -1),
        context_condition.reshape(1, -1),
        shift_weight,
        scale_weight,
        gate_weight,
        context,
    )
    parts = exchanged(parts, "z")
    latent_x = from_all_x(latent)
    sums = jnp.sum(parts[:, share:, : 5 * columns].astype(F32), axis=(0, 1)).reshape(1, -1)
    planes = exchanged(copies(sums, PLANE), PLANE)
    ctx_x = from_all_x(parts[:, :share].reshape(nz * share, width))
    latent_c = swapped(latent_x)
    ctx_c = swapped(ctx_x)
    pair_weight = jnp.concatenate([key_matrix, value_matrix], axis=1)
    cosine, sine = tables(place * group_rows + jnp.arange(group_rows, dtype=jnp.int32))
    ctx_pairs = pl.pallas_call(
        context_kernel,
        out_shape=shape_of((ny, nx * nc * nz * share, 2 * HEAD_DIM), BF16),
        in_specs=[VMEM] * 5,
        out_specs=VMEM,
        scratch_shapes=[pltpu.VMEM((nx * nc * nz * share, width), BF16)],
        name="context_pairs",
    )(ctx_x, ctx_c, planes, gain, pair_weight)
    ctx_pairs = exchanged(ctx_pairs, "y")
    sources = (lax.axis_index("x").astype(jnp.int32) - jnp.array(SHIFTS, jnp.int32)) % nx
    bases = jnp.concatenate([2 * sources + core, 2 * sources + 1 - core]) * rows
    queries, pairs = pl.pallas_call(
        qkv_kernel,
        out_shape=(
            shape_of((group_rows, 2 * HEAD_DIM), BF16),
            shape_of((group_rows, 2 * HEAD_DIM), BF16),
        ),
        in_specs=[SMEM] + [VMEM] * 8,
        out_specs=(VMEM, VMEM),
        scratch_shapes=[pltpu.VMEM((group_rows, width), BF16)],
        name="qkv",
    )(bases, latent_x, latent_c, planes, gain, query_weight, pair_weight, cosine, sine)
    count = nz * ny
    forward = [(i, i + 1) for i in range(count - 1)]
    backward = [(i + 1, i) for i in range(count - 1)]
    low = lax.ppermute(pairs[group_rows - WINDOW_REACH :], SP, forward)
    high = lax.ppermute(pairs[:WINDOW_REACH], SP, backward)
    where = jnp.stack(
        [core, (place == 0).astype(jnp.int32), (place == count - 1).astype(jnp.int32)]
    )
    half = group_rows // nc
    keep, send = pl.pallas_call(
        attention_kernel,
        out_shape=(
            shape_of((half, 2 * HEAD_DIM), BF16),
            shape_of((half, width), BF16),
        ),
        in_specs=[SMEM] * 2 + [VMEM] * 6,
        out_specs=(VMEM, VMEM),
        scratch_shapes=[
            pltpu.VMEM((group_rows + 2 * WINDOW_REACH, 2 * HEAD_DIM), BF16),
            pltpu.VMEM((group_rows, 2 * HEAD_DIM), BF16),
            pltpu.VMEM((half, 2 * HEAD_DIM), BF16),
        ],
        name="attention",
    )(where, sink_logit_head, queries, low, pairs, high, ctx_pairs, out_weight)
    got = swapped(send)
    paired = pl.pallas_call(
        pair_kernel,
        out_shape=shape_of((nx, rows, width), BF16),
        in_specs=[VMEM] * 3,
        out_specs=VMEM,
        name="pair",
    )(keep, out_weight, got)
    mixed = exchanged(paired, "x")
    return pl.pallas_call(
        final_kernel,
        out_shape=shape_of((rows, width), BF16),
        in_specs=[VMEM] * 3,
        out_specs=VMEM,
        name="final",
    )(latent, mixed, planes)


def solution(mesh):
    torus = Mesh(mesh.devices.reshape(16, 4, 4, 2), ALL)

    return jax.shard_map(
        shards,
        mesh=torus,
        in_specs=(
            P(ALL, None),
            P(SP),
            P(SP),
            P(SP, None),
            P(),
            P(SP, TP),
            P(SP, TP),
            P(SP, TP),
            P(None, TP),
            P(None, TP),
            P(None, TP),
            P(TP),
            P(TP, None),
        ),
        out_specs=P(ALL, None),
        check_vma=False,
    )
```

```python
import jax
import jax.numpy as jnp
from jax import lax
from jax.experimental import pallas as pl
from jax.experimental.pallas import tpu as pltpu
from jax.sharding import Mesh
from jax.sharding import PartitionSpec as P

HEAD_DIM = 128
WINDOW_REACH = 128
GRID_W = 64
SP = ("z", "y")
TP = ("x", "c")
PLANE = ("y", "x", "c")
ALL = ("z", "y", "x", "c")
NORM_EPS = 1e-05
MASKED_SCORE = -1e30
LOG2_E = 1.4426950408889634
CHUNK = 16


VMEM = pl.BlockSpec(memory_space=pltpu.VMEM)
SMEM = pl.BlockSpec(memory_space=pltpu.SMEM)
F32 = jnp.float32
BF16 = jnp.bfloat16


def shape_of(shape, dtype):
    return jax.ShapeDtypeStruct(shape, dtype)


def copies(x, axis):
    return jnp.broadcast_to(x[None], (lax.axis_size(axis), *x.shape))


def exchanged(blocks, axis):
    return lax.all_to_all(blocks, axis, 0, 0, tiled=True)


def dot(a, b):
    return jnp.dot(a, b, preferred_element_type=F32)


def row_vector(planes_ref, index, columns):
    count = planes_ref.shape[0] // 4
    cut = pl.ds(index * columns, columns)
    pieces = []
    for t in range(count):
        piece = planes_ref[t, :, cut]
        for y in range(1, 4):
            piece = piece + planes_ref[y * count + t, :, cut]
        pieces.append(piece)
    return jnp.concatenate(pieces, axis=1)


def parts_kernel(cond_ref, ctx_cond_ref, shift_ref, scale_ref, gate_ref, out_ref):
    def active(ref):
        v = ref[...]
        return (v / (1.0 + jnp.exp(-v))).astype(BF16)

    both = jnp.concatenate([active(cond_ref), active(ctx_cond_ref)], axis=0)
    both = jnp.concatenate([both, jnp.zeros((14, both.shape[1]), BF16)], axis=0)
    shift = dot(both, shift_ref[...])
    scale = dot(both, scale_ref[...])
    gate = dot(both, gate_ref[...])
    row = jnp.concatenate([shift[0:1], shift[1:2], scale[0:1], scale[1:2], gate[0:1]], axis=1)
    for i in range(out_ref.shape[0]):
        out_ref[i] = row


def normed_rows(ref, x, start, multiplier, shift):
    rows = ref[x, pl.ds(start, CHUNK), :].astype(F32)
    mean = jnp.mean(rows * rows, axis=-1, keepdims=True)
    return (rows * lax.rsqrt(mean + NORM_EPS) * multiplier + shift).astype(BF16)


def turned(u, cosine, sine):
    lane = lax.broadcasted_iota(jnp.int32, u.shape, 1)
    first = (lane % 64) < 32
    swapped = jnp.where(first, pltpu.roll(u, 96, 1), pltpu.roll(u, 32, 1))
    return u * cosine + swapped * sine


def qkv_kernel(
    base_ref, own_ref, other_ref, planes_ref, gain_ref, wq_ref, wkv_ref, cos_ref, sin_ref,
    q_ref, kv_ref, hidden_ref,
):
    columns = wq_ref.shape[1]
    shift = row_vector(planes_ref, 0, columns)
    multiplier = gain_ref[...] * (1.0 + row_vector(planes_ref, 2, columns))
    count, rows, _ = own_ref.shape
    steps = rows // CHUNK

    def step(i, carry):
        x = i // steps
        start = pl.multiple_of((i % steps) * CHUNK, CHUNK)
        at = pl.multiple_of(base_ref[x] + start, CHUNK)
        hidden_ref[pl.ds(at, CHUNK), :] = normed_rows(own_ref, x, start, multiplier, shift)
        at = pl.multiple_of(base_ref[count + x] + start, CHUNK)
        hidden_ref[pl.ds(at, CHUNK), :] = normed_rows(other_ref, x, start, multiplier, shift)
        return carry

    lax.fori_loop(0, count * steps, step, 0)
    block = 384
    for at in range(0, hidden_ref.shape[0], block):
        cut = slice(at, at + block)
        hidden = hidden_ref[cut, :]
        cosine, sine = cos_ref[cut, :], sin_ref[cut, :]
        queries = dot(hidden, wq_ref[...])
        q_ref[cut, :HEAD_DIM] = turned(queries[:, :HEAD_DIM], cosine, sine).astype(BF16)
        q_ref[cut, HEAD_DIM:] = turned(queries[:, HEAD_DIM:], cosine, sine).astype(BF16)
        pairs = dot(hidden, wkv_ref[...])
        kv_ref[cut, :HEAD_DIM] = turned(pairs[:, :HEAD_DIM], cosine, sine).astype(BF16)
        kv_ref[cut, HEAD_DIM:] = pairs[:, HEAD_DIM:].astype(BF16)


def context_kernel(ctx_ref, planes_ref, gain_ref, wkv_ref, out_ref):
    columns = wkv_ref.shape[1]
    shift = row_vector(planes_ref, 1, columns)
    multiplier = gain_ref[...] * (1.0 + row_vector(planes_ref, 3, columns))
    rows = ctx_ref[...].astype(F32)
    mean = jnp.mean(rows * rows, axis=-1, keepdims=True)
    hidden = (rows * lax.rsqrt(mean + NORM_EPS) * multiplier + shift).astype(BF16)
    pairs = dot(hidden, wkv_ref[...]).astype(BF16)
    for z in range(out_ref.shape[0]):
        out_ref[z] = pairs


def attention_kernel(
    place_ref, sink_ref, q_ref, low_ref, kv_ref, high_ref, ctx_ref, attended_ref, padded_ref,
):
    reach = WINDOW_REACH
    total = kv_ref.shape[0]
    first, last = place_ref[0], place_ref[1]
    padded_ref[:reach, :] = low_ref[...]
    padded_ref[reach : reach + total, :] = kv_ref[...]
    padded_ref[reach + total :, :] = high_ref[...]
    ctx_keys, ctx_values = ctx_ref[:, :HEAD_DIM], ctx_ref[:, HEAD_DIM:]
    factor = HEAD_DIM ** (-0.5) * LOG2_E
    row = lax.broadcasted_iota(jnp.int32, (2 * reach, 1), 0)
    sink = jnp.where(row < reach, sink_ref[0], sink_ref[1]) * LOG2_E
    position = lax.broadcasted_iota(jnp.int32, (2 * reach, 3 * reach), 0) % reach
    column = lax.broadcasted_iota(jnp.int32, (2 * reach, 3 * reach), 1)
    band = (column >= position) & (column <= position + 2 * reach)
    blocks = total // reach
    contract = (((1,), (1,)), ((), ()))

    def step(b, carry):
        at = pl.multiple_of(b * reach, reach)
        both = q_ref[pl.ds(at, reach), :]
        queries = jnp.concatenate([both[:, :HEAD_DIM], both[:, HEAD_DIM:]], axis=0)
        keys = padded_ref[pl.ds(at, 3 * reach), :HEAD_DIM]
        values = padded_ref[pl.ds(at, 3 * reach), HEAD_DIM:]
        lowest = jnp.where(b == 0, first * reach, 0)
        highest = jnp.where(b == blocks - 1, (3 - last) * reach, 3 * reach)
        allowed = band & (column >= lowest) & (column < highest)
        near = lax.dot_general(queries, keys, contract, preferred_element_type=F32) * factor
        near = jnp.where(allowed, near, MASKED_SCORE)
        far = lax.dot_general(queries, ctx_keys, contract, preferred_element_type=F32) * factor
        top = jnp.maximum(
            jnp.max(near, axis=-1, keepdims=True), jnp.max(far, axis=-1, keepdims=True)
        )
        top = jnp.maximum(top, sink)
        near = jnp.exp2(near - top)
        far = jnp.exp2(far - top)
        share = (
            jnp.sum(near, axis=-1, keepdims=True)
            + jnp.sum(far, axis=-1, keepdims=True)
            + jnp.exp2(sink - top)
        )
        mixed = dot(near.astype(BF16), values) + dot(far.astype(BF16), ctx_values)
        mixed = (mixed / share).astype(BF16)
        attended_ref[pl.ds(at, reach), :HEAD_DIM] = mixed[:reach]
        attended_ref[pl.ds(at, reach), HEAD_DIM:] = mixed[reach:]
        return carry

    lax.fori_loop(0, blocks, step, 0)


def project_kernel(
    source_ref, attended_ref, w0_ref, w1_ref, w2_ref, w3_ref, send_ref, keep_ref, rows_ref
):
    weights = (w0_ref, w1_ref, w2_ref, w3_ref)
    core = source_ref[4]
    rows = send_ref.shape[0]
    deep = attended_ref.shape[2]
    mine = pl.multiple_of(core * rows, CHUNK)
    theirs = pl.multiple_of((1 - core) * rows, CHUNK)
    for j in range(4):
        cut = slice(j * deep, (j + 1) * deep)
        rows_ref[:rows, cut] = attended_ref[source_ref[j], pl.ds(theirs, rows), :]
        rows_ref[rows:, cut] = attended_ref[source_ref[j], pl.ds(mine, rows), :]
    width = 512
    for n in range(0, send_ref.shape[1], width):
        cut = slice(n, n + width)
        total = dot(rows_ref[:, :deep], w0_ref[:, cut])
        for j in range(1, 4):
            total = total + dot(rows_ref[:, j * deep : (j + 1) * deep], weights[j][:, cut])
        send_ref[:, cut] = total[:rows].astype(BF16)
        keep_ref[:, cut] = total[rows:]


def final_kernel(latent_ref, keep_ref, got_ref, planes_ref, out_ref):
    gate = row_vector(planes_ref, 4, planes_ref.shape[2] // 5)

    def step(i, carry):
        cut = pl.ds(pl.multiple_of(i * CHUNK, CHUNK), CHUNK)
        mixed = keep_ref[cut, :] + got_ref[cut, :].astype(F32)
        out_ref[cut, :] = (latent_ref[cut, :].astype(F32) + gate * mixed).astype(BF16)
        return carry

    lax.fori_loop(0, latent_ref.shape[0] // CHUNK, step, 0)


SHIFTS = (0, 1, 3, 2)


def from_other_x(block):
    got = []
    for shift in SHIFTS[1:]:
        got.append(lax.ppermute(block, "x", [(i, (i + shift) % 4) for i in range(4)]))
    return got


def swapped(x):
    return lax.ppermute(x, "c", [(0, 1), (1, 0)])


def tables(position):
    inv_freq = 10000.0 ** (-jnp.arange(0, HEAD_DIM // 2, 2, dtype=F32) / (HEAD_DIM // 2))
    by_row = (position // GRID_W).astype(F32)[:, None] * inv_freq
    by_col = (position % GRID_W).astype(F32)[:, None] * inv_freq
    angles = jnp.concatenate([by_row, by_row, by_col, by_col], axis=1)
    sign = jnp.where((jnp.arange(HEAD_DIM) % 64) < 32, -1.0, 1.0).astype(F32)
    return jnp.cos(angles), jnp.sin(angles) * sign


def shards(
    latent,
    condition,
    context_condition,
    context,
    norm_gain,
    shift_weight,
    scale_weight,
    gate_weight,
    query_weight,
    key_matrix,
    value_matrix,
    sink_logit_head,
    out_weight,
):
    nz, ny, nx, nc = (lax.axis_size(a) for a in ALL)
    rows, width = latent.shape
    group_rows = rows * nx * nc
    columns = shift_weight.shape[1]
    place = lax.axis_index(SP)
    core = lax.axis_index("c").astype(jnp.int32)
    gain = norm_gain.reshape(1, width)
    at_x = lax.axis_index("x").astype(jnp.int32)
    parts = pl.pallas_call(
        parts_kernel,
        out_shape=shape_of((nz, 1, 5 * columns), F32),
        in_specs=[VMEM] * 5,
        out_specs=VMEM,
        name="parts",
    )(
        condition.reshape(1, -1),
        context_condition.reshape(1, -1),
        shift_weight,
        scale_weight,
        gate_weight,
    )
    parts = exchanged(parts, "z")
    latent_others = from_other_x(latent)
    pair_weight = jnp.concatenate([key_matrix, value_matrix], axis=1)
    cosine, sine = tables(place * group_rows + jnp.arange(group_rows, dtype=jnp.int32))
    planes = exchanged(copies(jnp.sum(parts, axis=0), PLANE), PLANE)
    out_others = from_other_x(out_weight)
    latent_x = jnp.stack([latent, *latent_others])
    latent_c = swapped(latent_x)
    ctx_rows = context.shape[0]
    pairs = pl.pallas_call(
        context_kernel,
        out_shape=shape_of((nz, ctx_rows, 2 * HEAD_DIM), BF16),
        in_specs=[VMEM] * 4,
        out_specs=VMEM,
        name="context_pairs",
    )(context, planes, gain, pair_weight)
    ctx_z = exchanged(pairs, "z")
    ctx_pairs = exchanged(copies(ctx_z.reshape(nz * ctx_rows, -1), "y"), "y")
    ctx_pairs = ctx_pairs.reshape(-1, 2 * HEAD_DIM)
    sources = (at_x - jnp.array(SHIFTS, jnp.int32)) % nx
    bases = jnp.concatenate([2 * sources + core, 2 * sources + 1 - core]) * rows
    queries, pairs = pl.pallas_call(
        qkv_kernel,
        out_shape=(
            shape_of((group_rows, 2 * HEAD_DIM), BF16),
            shape_of((group_rows, 2 * HEAD_DIM), BF16),
        ),
        in_specs=[SMEM] + [VMEM] * 8,
        out_specs=(VMEM, VMEM),
        scratch_shapes=[pltpu.VMEM((group_rows, width), BF16)],
        name="qkv",
    )(bases, latent_x, latent_c, planes, gain, query_weight, pair_weight, cosine, sine)
    count = nz * ny
    forward = [(i, i + 1) for i in range(count - 1)]
    low = lax.ppermute(pairs[group_rows - WINDOW_REACH :], SP, forward)
    backward = [(i + 1, i) for i in range(count - 1)]
    high = lax.ppermute(pairs[:WINDOW_REACH], SP, backward)
    where = jnp.stack([(place == 0).astype(jnp.int32), (place == count - 1).astype(jnp.int32)])
    attended = pl.pallas_call(
        attention_kernel,
        out_shape=shape_of((group_rows, 2 * HEAD_DIM), BF16),
        in_specs=[SMEM] * 2 + [VMEM] * 5,
        out_specs=VMEM,
        scratch_shapes=[
            pltpu.VMEM((group_rows + 2 * WINDOW_REACH, 2 * HEAD_DIM), BF16),
        ],
        name="attention",
    )(where, sink_logit_head, queries, low, pairs, high, ctx_pairs)
    attended = exchanged(attended.reshape(nx, nc * rows, 2 * HEAD_DIM), "x")
    send, keep = pl.pallas_call(
        project_kernel,
        out_shape=(shape_of((rows, width), BF16), shape_of((rows, width), F32)),
        in_specs=[SMEM] + [VMEM] * 5,
        out_specs=(VMEM, VMEM),
        scratch_shapes=[pltpu.VMEM((nc * rows, nx * 2 * HEAD_DIM), BF16)],
        name="project",
    )(jnp.concatenate([sources, core[None]]), attended, out_weight, *out_others)
    got = swapped(send)
    return pl.pallas_call(
        final_kernel,
        out_shape=shape_of((rows, width), BF16),
        in_specs=[VMEM] * 4,
        out_specs=VMEM,
        name="final",
    )(latent, keep, got, planes)


def solution(mesh):
    torus = Mesh(mesh.devices.reshape(16, 4, 4, 2), ALL)

    return jax.shard_map(
        shards,
        mesh=torus,
        in_specs=(
            P(ALL, None),
            P(SP),
            P(SP),
            P(SP, None),
            P(),
            P(SP, TP),
            P(SP, TP),
            P(SP, TP),
            P(None, TP),
            P(None, TP),
            P(None, TP),
            P(TP),
            P(TP, None),
        ),
        out_specs=P(ALL, None),
        check_vma=False,
    )
```

```python
import jax
import jax.numpy as jnp
from jax import lax
from jax.experimental import pallas as pl
from jax.experimental.pallas import tpu as pltpu
from jax.sharding import Mesh
from jax.sharding import PartitionSpec as P

HEAD_DIM = 128
WINDOW_REACH = 128
GRID_W = 64
SP = ("z", "y")
TP = ("x", "c")
PLANE = ("y", "x", "c")
ALL = ("z", "y", "x", "c")
NORM_EPS = 1e-05
MASKED_SCORE = -1e30
LOG2_E = 1.4426950408889634
CHUNK = 16
SHIFTS = (0, 1, 3, 2)


VMEM = pl.BlockSpec(memory_space=pltpu.VMEM)
SMEM = pl.BlockSpec(memory_space=pltpu.SMEM)
F32 = jnp.float32
BF16 = jnp.bfloat16


def shape_of(shape, dtype):
    return jax.ShapeDtypeStruct(shape, dtype)


def vmem(mib):
    return pltpu.CompilerParams(vmem_limit_bytes=mib * 2**20)


def held(*arrays):
    return [pltpu.with_memory_space_constraint(a, pltpu.VMEM) for a in arrays]


def exchanged(blocks, axis):
    return lax.all_to_all(blocks, axis, 0, 0, tiled=True)


def dot(a, b):
    return jnp.dot(a, b, preferred_element_type=F32)


def row_vector(planes_ref, index, columns):
    count = planes_ref.shape[0] // 4
    cut = pl.ds(index * columns, columns)
    pieces = []
    for t in range(count):
        piece = planes_ref[t, :, cut]
        for y in range(1, 4):
            piece = piece + planes_ref[y * count + t, :, cut]
        pieces.append(piece)
    return jnp.concatenate(pieces, axis=1)


def parts_kernel(cond_ref, ctx_cond_ref, shift_ref, scale_ref, gate_ref, out_ref):
    def active(ref):
        v = ref[...]
        return (v / (1.0 + jnp.exp(-v))).astype(BF16)

    both = jnp.concatenate([active(cond_ref), active(ctx_cond_ref)], axis=0)
    both = jnp.concatenate([both, jnp.zeros((14, both.shape[1]), BF16)], axis=0)
    shift = dot(both, shift_ref[...])
    scale = dot(both, scale_ref[...])
    gate = dot(both, gate_ref[...])
    row = jnp.concatenate([shift[0:1], shift[1:2], scale[0:1], scale[1:2], gate[0:1]], axis=1)
    for i in range(out_ref.shape[0]):
        out_ref[i] = row


def normed_rows(ref, x, start, multiplier, shift):
    rows = ref[x, pl.ds(start, CHUNK), :].astype(F32)
    mean = jnp.mean(rows * rows, axis=-1, keepdims=True)
    return (rows * lax.rsqrt(mean + NORM_EPS) * multiplier + shift).astype(BF16)


def turned(u, cosine, sine):
    lane = lax.broadcasted_iota(jnp.int32, u.shape, 1)
    first = (lane % 64) < 32
    swapped = jnp.where(first, pltpu.roll(u, 96, 1), pltpu.roll(u, 32, 1))
    return u * cosine + swapped * sine


def sum_kernel(parts_ref, out_ref):
    total = parts_ref[0]
    for z in range(1, parts_ref.shape[0]):
        total = total + parts_ref[z]
    for p in range(out_ref.shape[0]):
        out_ref[p] = total


def qkv_kernel(
    place_ref, own_ref, other_ref, planes_ref, gain_ref, wq_ref, wk_ref, wv_ref, row_ref, col_ref,
    q_ref, kv_ref, top_ref, bottom_ref, hidden_ref, wkv_ref,
):
    columns = wq_ref.shape[1]
    shift = row_vector(planes_ref, 0, columns)
    multiplier = gain_ref[...] * (1.0 + row_vector(planes_ref, 2, columns))
    wkv_ref[:, :HEAD_DIM] = wk_ref[...]
    wkv_ref[:, HEAD_DIM:] = wv_ref[...]
    _, rows, _ = own_ref.shape
    at_x, core = place_ref[0], place_ref[1]
    for x, shift_x in enumerate(SHIFTS):
        source = lax.rem(at_x - shift_x + 4, 4)
        mine = (2 * source + core) * rows
        theirs = (2 * source + 1 - core) * rows

        def step(i, carry, x=x, mine=mine, theirs=theirs):
            start = pl.multiple_of(i * CHUNK, CHUNK)
            at = pl.multiple_of(mine + start, CHUNK)
            hidden_ref[pl.ds(at, CHUNK), :] = normed_rows(own_ref, x, start, multiplier, shift)
            at = pl.multiple_of(theirs + start, CHUNK)
            hidden_ref[pl.ds(at, CHUNK), :] = normed_rows(other_ref, x, start, multiplier, shift)
            return carry

        lax.fori_loop(0, rows // CHUNK, step, 0, unroll=2)
    block = 384
    lane = lax.broadcasted_iota(jnp.int32, (GRID_W, HEAD_DIM), 1) < 64
    col = col_ref[...]
    col_turned = pltpu.roll(col, 64, 1)
    row_turned = pltpu.roll(row_ref[...], 64, 1)
    factor = HEAD_DIM ** (-0.5) * LOG2_E
    for at in range(0, hidden_ref.shape[0], block):
        cut = slice(at, at + block)
        hidden = hidden_ref[cut, :]
        lines = range(at // GRID_W, (at + block) // GRID_W)
        cosine = jnp.concatenate(
            [jnp.where(lane, row_ref[g : g + 1, :], col_turned) for g in lines], axis=0
        )
        sine = jnp.concatenate(
            [jnp.where(lane, row_turned[g : g + 1, :], col) for g in lines], axis=0
        )
        queries = dot(hidden, wq_ref[...])
        for h in range(2):
            part = slice(h * HEAD_DIM, (h + 1) * HEAD_DIM)
            q_ref[cut, part] = (turned(queries[:, part], cosine, sine) * factor).astype(BF16)
        pairs = dot(hidden, wkv_ref[...])
        kv_ref[cut, :HEAD_DIM] = turned(pairs[:, :HEAD_DIM], cosine, sine).astype(BF16)
        kv_ref[cut, HEAD_DIM:] = pairs[:, HEAD_DIM:].astype(BF16)
    top_ref[...] = kv_ref[:WINDOW_REACH, :]
    bottom_ref[...] = kv_ref[hidden_ref.shape[0] - WINDOW_REACH :, :]


def context_kernel(ctx_ref, planes_ref, gain_ref, wk_ref, wv_ref, out_ref):
    columns = planes_ref.shape[2] // 5
    shift = row_vector(planes_ref, 1, columns)
    multiplier = gain_ref[...] * (1.0 + row_vector(planes_ref, 3, columns))
    rows = ctx_ref[...].astype(F32)
    mean = jnp.mean(rows * rows, axis=-1, keepdims=True)
    hidden = (rows * lax.rsqrt(mean + NORM_EPS) * multiplier + shift).astype(BF16)
    pairs = jnp.concatenate([dot(hidden, wk_ref[...]), dot(hidden, wv_ref[...])], axis=1)
    pairs = pairs.astype(BF16)
    for p in range(out_ref.shape[0]):
        out_ref[p] = pairs


def attention_kernel(
    place_ref, sink_ref, q_ref, low_ref, kv_ref, high_ref, ctx_ref, attended_ref,
    keys_ref, values_ref, ctx_values_ref,
):
    reach = WINDOW_REACH
    total = kv_ref.shape[0]
    first, last = place_ref[2], place_ref[3]
    for ref, at in ((low_ref, 0), (kv_ref, reach), (high_ref, reach + total)):
        cut = slice(at, at + ref.shape[0])
        keys_ref[cut, :] = ref[:, :HEAD_DIM]
        values_ref[cut, :HEAD_DIM] = ref[:, HEAD_DIM:]
    values_ref[:, HEAD_DIM:] = jnp.ones(keys_ref.shape, BF16)
    ctx_values_ref[:, :HEAD_DIM] = ctx_ref[:, HEAD_DIM:]
    ctx_values_ref[:, HEAD_DIM:] = jnp.ones((ctx_ref.shape[0], HEAD_DIM), BF16)
    row = lax.broadcasted_iota(jnp.int32, (2 * reach, 1), 0)
    sink = jnp.where(row < reach, sink_ref[0], sink_ref[1]) * LOG2_E
    position = lax.broadcasted_iota(jnp.int32, (2 * reach, 3 * reach), 0) % reach
    column = lax.broadcasted_iota(jnp.int32, (2 * reach, 3 * reach), 1)
    band = (column >= position) & (column <= position + 2 * reach)
    blocks = total // reach
    contract = (((1,), (1,)), ((), ()))

    def step(b, carry):
        at = pl.multiple_of(b * reach, reach)
        both = q_ref[pl.ds(at, reach), :]
        queries = jnp.concatenate([both[:, :HEAD_DIM], both[:, HEAD_DIM:]], axis=0)
        keys = keys_ref[pl.ds(at, 3 * reach), :]
        values = values_ref[pl.ds(at, 3 * reach), :]
        lowest = jnp.where(b == 0, first * reach, 0)
        highest = jnp.where(b == blocks - 1, (3 - last) * reach, 3 * reach)
        allowed = band & (column >= lowest) & (column < highest)
        near = lax.dot_general(queries, keys, contract, preferred_element_type=F32)
        near = jnp.where(allowed, near, MASKED_SCORE)
        far = lax.dot_general(
            queries, ctx_ref[:, :HEAD_DIM], contract, preferred_element_type=F32
        )
        top = jnp.maximum(
            jnp.max(near, axis=-1, keepdims=True), jnp.max(far, axis=-1, keepdims=True)
        )
        top = jnp.maximum(top, sink)
        near = jnp.exp2(near - top).astype(BF16)
        far = jnp.exp2(far - top).astype(BF16)
        mixed = dot(near, values) + dot(far, ctx_values_ref[...])
        share = mixed[:, HEAD_DIM:] + jnp.exp2(sink - top)
        mixed = (mixed[:, :HEAD_DIM] / share).astype(BF16)
        attended_ref[pl.ds(at, reach), :HEAD_DIM] = mixed[:reach]
        attended_ref[pl.ds(at, reach), HEAD_DIM:] = mixed[reach:]
        return carry

    lax.fori_loop(0, blocks, step, 0, unroll=2)


def project_kernel(
    place_ref, attended_ref, w0_ref, w1_ref, w2_ref, w3_ref, send_ref, keep_ref, rows_ref
):
    weights = (w0_ref, w1_ref, w2_ref, w3_ref)
    at_x, core = place_ref[0], place_ref[1]
    rows = send_ref.shape[0]
    deep = attended_ref.shape[2]
    mine = pl.multiple_of(core * rows, CHUNK)
    theirs = pl.multiple_of((1 - core) * rows, CHUNK)
    for j, shift_x in enumerate(SHIFTS):
        source = lax.rem(at_x - shift_x + 4, 4)
        cut = slice(j * deep, (j + 1) * deep)
        rows_ref[:rows, cut] = attended_ref[source, pl.ds(theirs, rows), :]
        rows_ref[rows:, cut] = attended_ref[source, pl.ds(mine, rows), :]
    width = 512
    for n in range(0, send_ref.shape[1], width):
        cut = slice(n, n + width)
        total = dot(rows_ref[:, :deep], w0_ref[:, cut])
        for j in range(1, 4):
            total = total + dot(rows_ref[:, j * deep : (j + 1) * deep], weights[j][:, cut])
        send_ref[:, cut] = total[:rows].astype(BF16)
        keep_ref[:, cut] = total[rows:]


def final_kernel(latent_ref, keep_ref, got_ref, planes_ref, out_ref):
    gate = row_vector(planes_ref, 4, planes_ref.shape[2] // 5)

    def step(i, carry):
        cut = pl.ds(pl.multiple_of(i * CHUNK, CHUNK), CHUNK)
        mixed = keep_ref[cut, :] + got_ref[cut, :].astype(F32)
        out_ref[cut, :] = (latent_ref[cut, :].astype(F32) + gate * mixed).astype(BF16)
        return carry

    lax.fori_loop(0, latent_ref.shape[0] // CHUNK, step, 0)


def from_other_x(block):
    got = []
    for shift in SHIFTS[1:]:
        got.append(lax.ppermute(block, "x", [(i, (i + shift) % 4) for i in range(4)]))
    return got


def swapped(x):
    return lax.ppermute(x, "c", [(0, 1), (1, 0)])


def tables(first_line, lines):
    inv_freq = 10000.0 ** (-jnp.arange(0, HEAD_DIM // 2, 2, dtype=F32) / (HEAD_DIM // 2))
    at = jnp.concatenate([first_line + jnp.arange(lines), jnp.arange(GRID_W)])
    angles = at.astype(F32)[:, None] * inv_freq
    cosine, sine = jnp.cos(angles), jnp.sin(angles)
    table = jnp.concatenate([cosine, cosine, -sine, sine], axis=1)
    return table[:lines], table[lines:]


def shards(
    latent,
    condition,
    context_condition,
    context,
    norm_gain,
    shift_weight,
    scale_weight,
    gate_weight,
    query_weight,
    key_matrix,
    value_matrix,
    sink_logit_head,
    out_weight,
):
    nz, ny, nx, nc = (lax.axis_size(a) for a in ALL)
    rows, width = latent.shape
    group_rows = rows * nx * nc
    columns = shift_weight.shape[1]
    place = lax.axis_index(SP)
    gain = norm_gain.reshape(1, width)
    parts = pl.pallas_call(
        parts_kernel,
        out_shape=shape_of((nz, 1, 5 * columns), F32),
        in_specs=[VMEM] * 5,
        out_specs=VMEM,
        name="parts",
        compiler_params=vmem(6),
    )(
        condition.reshape(1, -1),
        context_condition.reshape(1, -1),
        shift_weight,
        scale_weight,
        gate_weight,
    )
    parts = exchanged(parts, "z")
    latent_others = from_other_x(latent)
    lines, cols = tables(place * (group_rows // GRID_W), group_rows // GRID_W)
    count = nz * ny
    where = jnp.stack(
        [
            lax.axis_index("x").astype(jnp.int32),
            lax.axis_index("c").astype(jnp.int32),
            (place == 0).astype(jnp.int32),
            (place == count - 1).astype(jnp.int32),
        ]
    )
    members = ny * nx * nc
    sums = pl.pallas_call(
        sum_kernel,
        out_shape=shape_of((members, 1, 5 * columns), F32),
        in_specs=[VMEM],
        out_specs=VMEM,
        name="sums",
        compiler_params=vmem(4),
    )(*held(parts))
    planes = exchanged(sums, PLANE)
    out_others = from_other_x(out_weight)
    latent_x = jnp.stack([latent, *latent_others])
    latent_c = swapped(latent_x)
    ctx_rows = context.shape[0]
    pairs = pl.pallas_call(
        context_kernel,
        out_shape=shape_of((count, ctx_rows, 2 * HEAD_DIM), BF16),
        in_specs=[VMEM] * 5,
        out_specs=VMEM,
        name="context_pairs",
        compiler_params=vmem(8),
    )(*held(context, planes, gain, key_matrix, value_matrix))
    ctx_pairs = exchanged(pairs, SP).reshape(-1, 2 * HEAD_DIM)
    wide = (group_rows, 2 * HEAD_DIM)
    edge = (WINDOW_REACH, 2 * HEAD_DIM)
    queries, pairs, top, bottom = pl.pallas_call(
        qkv_kernel,
        out_shape=[pltpu.VMEM(shape, BF16) for shape in (wide, wide, edge, edge)],
        in_specs=[SMEM] + [VMEM] * 9,
        out_specs=[VMEM] * 4,
        scratch_shapes=[
            pltpu.VMEM((group_rows, width), BF16),
            pltpu.VMEM((width, 2 * HEAD_DIM), BF16),
        ],
        name="qkv",
        compiler_params=vmem(20),
    )(
        where,
        *held(latent_x, latent_c, planes, gain),
        *held(query_weight, key_matrix, value_matrix, lines, cols),
    )
    low = lax.ppermute(bottom, SP, [(i, i + 1) for i in range(count - 1)])
    high = lax.ppermute(top, SP, [(i + 1, i) for i in range(count - 1)])
    long = group_rows + 2 * WINDOW_REACH
    attended = pl.pallas_call(
        attention_kernel,
        out_shape=shape_of(wide, BF16),
        in_specs=[SMEM] * 2 + [VMEM] * 5,
        out_specs=VMEM,
        scratch_shapes=[
            pltpu.VMEM((long, HEAD_DIM), BF16),
            pltpu.VMEM((long, 2 * HEAD_DIM), BF16),
            pltpu.VMEM((count * ctx_rows, 2 * HEAD_DIM), BF16),
        ],
        name="attention",
        compiler_params=vmem(16),
    )(where, sink_logit_head, *held(queries, low, pairs, high, ctx_pairs))
    attended = exchanged(attended.reshape(nx, nc * rows, 2 * HEAD_DIM), "x")
    send, keep = pl.pallas_call(
        project_kernel,
        out_shape=[pltpu.VMEM((rows, width), BF16), pltpu.VMEM((rows, width), F32)],
        in_specs=[SMEM] + [VMEM] * 5,
        out_specs=(VMEM, VMEM),
        scratch_shapes=[pltpu.VMEM((nc * rows, nx * 2 * HEAD_DIM), BF16)],
        name="project",
        compiler_params=vmem(14),
    )(where, *held(attended, out_weight, *out_others))
    got = swapped(send)
    return pl.pallas_call(
        final_kernel,
        out_shape=shape_of((rows, width), BF16),
        in_specs=[VMEM] * 4,
        out_specs=VMEM,
        name="final",
        compiler_params=vmem(8),
    )(*held(latent, keep, got, planes))


def solution(mesh):
    torus = Mesh(mesh.devices.reshape(16, 4, 4, 2), ALL)

    return jax.shard_map(
        shards,
        mesh=torus,
        in_specs=(
            P(ALL, None),
            P(SP),
            P(SP),
            P(SP, None),
            P(),
            P(SP, TP),
            P(SP, TP),
            P(SP, TP),
            P(None, TP),
            P(None, TP),
            P(None, TP),
            P(TP),
            P(TP, None),
        ),
        out_specs=P(ALL, None),
        check_vma=False,
    )
```

```python
import jax
import jax.numpy as jnp
from jax import lax
from jax.experimental import pallas as pl
from jax.experimental.pallas import tpu as pltpu
from jax.sharding import Mesh
from jax.sharding import PartitionSpec as P

HEAD_DIM = 128
WINDOW_REACH = 128
GRID_W = 64
SP = ("z", "y")
TP = ("x", "c")
PLANE = ("y", "x", "c")
ALL = ("z", "y", "x", "c")
NORM_EPS = 1e-05
MASKED_SCORE = -1e30
LOG2_E = 1.4426950408889634
CHUNK = 16
SHIFTS = (0, 1, 3, 2)


VMEM = pl.BlockSpec(memory_space=pltpu.VMEM)
SMEM = pl.BlockSpec(memory_space=pltpu.SMEM)
HBM = pl.BlockSpec(memory_space=pltpu.HBM)
F32 = jnp.float32
BF16 = jnp.bfloat16


def shape_of(shape, dtype):
    return jax.ShapeDtypeStruct(shape, dtype)


def copies(x, axis):
    return jnp.broadcast_to(x[None], (lax.axis_size(axis), *x.shape))


def vmem(mib):
    return pltpu.CompilerParams(vmem_limit_bytes=mib * 2**20)


def held(*arrays):
    return [pltpu.with_memory_space_constraint(a, pltpu.VMEM) for a in arrays]


def far(*arrays):
    return [pltpu.with_memory_space_constraint(a, pltpu.HBM) for a in arrays]


def exchanged(blocks, axis):
    return lax.all_to_all(blocks, axis, 0, 0, tiled=True)


def dot(a, b):
    return jnp.dot(a, b, preferred_element_type=F32)


def row_vector(planes_ref, index, columns):
    count = planes_ref.shape[0] // 4
    cut = pl.ds(index * columns, columns)
    pieces = []
    for t in range(count):
        piece = planes_ref[t, :, cut]
        for y in range(1, 4):
            piece = piece + planes_ref[y * count + t, :, cut]
        pieces.append(piece)
    return jnp.concatenate(pieces, axis=1)


def parts_kernel(cond_ref, ctx_cond_ref, shift_ref, scale_ref, gate_ref, out_ref):
    def active(ref):
        v = ref[...]
        return (v / (1.0 + jnp.exp(-v))).astype(BF16)

    both = jnp.concatenate([active(cond_ref), active(ctx_cond_ref)], axis=0)
    both = jnp.concatenate([both, jnp.zeros((14, both.shape[1]), BF16)], axis=0)
    shift = dot(both, shift_ref[...])
    scale = dot(both, scale_ref[...])
    gate = dot(both, gate_ref[...])
    row = jnp.concatenate([shift[0:1], shift[1:2], scale[0:1], scale[1:2], gate[0:1]], axis=1)
    for i in range(out_ref.shape[0]):
        out_ref[i] = row


def normed_rows(ref, x, start, multiplier, shift):
    rows = ref[x, pl.ds(start, CHUNK), :].astype(F32)
    mean = jnp.mean(rows * rows, axis=-1, keepdims=True)
    return (rows * lax.rsqrt(mean + NORM_EPS) * multiplier + shift).astype(BF16)


def turned(u, cosine, sine):
    lane = lax.broadcasted_iota(jnp.int32, u.shape, 1)
    first = (lane % 64) < 32
    swapped = jnp.where(first, pltpu.roll(u, 96, 1), pltpu.roll(u, 32, 1))
    return u * cosine + swapped * sine


def sum_kernel(parts_ref, out_ref):
    total = parts_ref[0]
    for z in range(1, parts_ref.shape[0]):
        total = total + parts_ref[z]
    for p in range(out_ref.shape[0]):
        out_ref[p] = total


def qkv_kernel(
    place_ref, own_ref, other_ref, planes_ref, gain_ref, wq_ref, wk_ref, wv_ref, row_ref, col_ref,
    q_ref, kv_ref, top_ref, bottom_ref, hidden_ref, wq_held_ref, wkv_ref, sems,
):
    columns = wq_ref.shape[1]
    loads = (
        pltpu.make_async_copy(wq_ref, wq_held_ref, sems.at[0]),
        pltpu.make_async_copy(wk_ref, wkv_ref.at[:, :HEAD_DIM], sems.at[1]),
        pltpu.make_async_copy(wv_ref, wkv_ref.at[:, HEAD_DIM:], sems.at[2]),
    )
    for load in loads:
        load.start()
    shift = row_vector(planes_ref, 0, columns)
    multiplier = gain_ref[...] * (1.0 + row_vector(planes_ref, 2, columns))
    _, rows, _ = own_ref.shape
    at_x, core = place_ref[0], place_ref[1]
    for x, shift_x in enumerate(SHIFTS):
        source = lax.rem(at_x - shift_x + 4, 4)
        mine = (2 * source + core) * rows
        theirs = (2 * source + 1 - core) * rows

        def step(i, carry, x=x, mine=mine, theirs=theirs):
            start = pl.multiple_of(i * CHUNK, CHUNK)
            at = pl.multiple_of(mine + start, CHUNK)
            hidden_ref[pl.ds(at, CHUNK), :] = normed_rows(own_ref, x, start, multiplier, shift)
            at = pl.multiple_of(theirs + start, CHUNK)
            hidden_ref[pl.ds(at, CHUNK), :] = normed_rows(other_ref, x, start, multiplier, shift)
            return carry

        lax.fori_loop(0, rows // CHUNK, step, 0, unroll=2)
    for load in loads:
        load.wait()
    block = 384
    lane = lax.broadcasted_iota(jnp.int32, (GRID_W, HEAD_DIM), 1) < 64
    col = col_ref[...]
    col_turned = pltpu.roll(col, 64, 1)
    row_turned = pltpu.roll(row_ref[...], 64, 1)
    factor = HEAD_DIM ** (-0.5) * LOG2_E
    for at in range(0, hidden_ref.shape[0], block):
        cut = slice(at, at + block)
        hidden = hidden_ref[cut, :]
        lines = range(at // GRID_W, (at + block) // GRID_W)
        cosine = jnp.concatenate(
            [jnp.where(lane, row_ref[g : g + 1, :], col_turned) for g in lines], axis=0
        )
        sine = jnp.concatenate(
            [jnp.where(lane, row_turned[g : g + 1, :], col) for g in lines], axis=0
        )
        queries = dot(hidden, wq_held_ref[...])
        for h in range(2):
            part = slice(h * HEAD_DIM, (h + 1) * HEAD_DIM)
            q_ref[cut, part] = (turned(queries[:, part], cosine, sine) * factor).astype(BF16)
        pairs = dot(hidden, wkv_ref[...])
        kv_ref[cut, :HEAD_DIM] = turned(pairs[:, :HEAD_DIM], cosine, sine).astype(BF16)
        kv_ref[cut, HEAD_DIM:] = pairs[:, HEAD_DIM:].astype(BF16)
    top_ref[...] = kv_ref[:WINDOW_REACH, :]
    bottom_ref[...] = kv_ref[hidden_ref.shape[0] - WINDOW_REACH :, :]


def context_kernel(ctx_ref, planes_ref, gain_ref, wk_ref, wv_ref, out_ref):
    columns = planes_ref.shape[2] // 5
    shift = row_vector(planes_ref, 1, columns)
    multiplier = gain_ref[...] * (1.0 + row_vector(planes_ref, 3, columns))
    rows = ctx_ref[...].astype(F32)
    mean = jnp.mean(rows * rows, axis=-1, keepdims=True)
    hidden = (rows * lax.rsqrt(mean + NORM_EPS) * multiplier + shift).astype(BF16)
    pairs = jnp.concatenate([dot(hidden, wk_ref[...]), dot(hidden, wv_ref[...])], axis=1)
    pairs = pairs.astype(BF16)
    for p in range(out_ref.shape[0]):
        out_ref[p] = pairs


def attention_kernel(
    place_ref, sink_ref, q_ref, low_ref, kv_ref, high_ref, ctx_ref, attended_ref,
    keys_ref, values_ref, ctx_values_ref,
):
    reach = WINDOW_REACH
    total = kv_ref.shape[0]
    first, last = place_ref[2], place_ref[3]
    for ref, at in ((low_ref, 0), (kv_ref, reach), (high_ref, reach + total)):
        cut = slice(at, at + ref.shape[0])
        keys_ref[cut, :] = ref[:, :HEAD_DIM]
        values_ref[cut, :HEAD_DIM] = ref[:, HEAD_DIM:]
    values_ref[:, HEAD_DIM:] = jnp.ones(keys_ref.shape, BF16)
    ctx_values_ref[:, :HEAD_DIM] = ctx_ref[:, HEAD_DIM:]
    ctx_values_ref[:, HEAD_DIM:] = jnp.ones((ctx_ref.shape[0], HEAD_DIM), BF16)
    row = lax.broadcasted_iota(jnp.int32, (2 * reach, 1), 0)
    sink = jnp.where(row < reach, sink_ref[0], sink_ref[1]) * LOG2_E
    position = lax.broadcasted_iota(jnp.int32, (2 * reach, 3 * reach), 0) % reach
    column = lax.broadcasted_iota(jnp.int32, (2 * reach, 3 * reach), 1)
    band = (column >= position) & (column <= position + 2 * reach)
    blocks = total // reach
    contract = (((1,), (1,)), ((), ()))

    def step(b, carry):
        at = pl.multiple_of(b * reach, reach)
        both = q_ref[pl.ds(at, reach), :]
        queries = jnp.concatenate([both[:, :HEAD_DIM], both[:, HEAD_DIM:]], axis=0)
        keys = keys_ref[pl.ds(at, 3 * reach), :]
        values = values_ref[pl.ds(at, 3 * reach), :]
        lowest = jnp.where(b == 0, first * reach, 0)
        highest = jnp.where(b == blocks - 1, (3 - last) * reach, 3 * reach)
        allowed = band & (column >= lowest) & (column < highest)
        near = lax.dot_general(queries, keys, contract, preferred_element_type=F32)
        near = jnp.where(allowed, near, MASKED_SCORE)
        far = lax.dot_general(
            queries, ctx_ref[:, :HEAD_DIM], contract, preferred_element_type=F32
        )
        top = jnp.maximum(
            jnp.max(near, axis=-1, keepdims=True), jnp.max(far, axis=-1, keepdims=True)
        )
        top = jnp.maximum(top, sink)
        near = jnp.exp2(near - top).astype(BF16)
        far = jnp.exp2(far - top).astype(BF16)
        mixed = dot(near, values) + dot(far, ctx_values_ref[...])
        share = mixed[:, HEAD_DIM:] + jnp.exp2(sink - top)
        mixed = (mixed[:, :HEAD_DIM] / share).astype(BF16)
        attended_ref[pl.ds(at, reach), :HEAD_DIM] = mixed[:reach]
        attended_ref[pl.ds(at, reach), HEAD_DIM:] = mixed[reach:]
        return carry

    lax.fori_loop(0, blocks, step, 0, unroll=2)


def project_kernel(
    place_ref, attended_ref, w0_ref, w1_ref, w2_ref, w3_ref, send_ref, keep_ref,
    rows_ref, total_ref, weights_ref, sems,
):
    loads = [
        pltpu.make_async_copy(w, weights_ref.at[j], sems.at[j])
        for j, w in enumerate((w0_ref, w1_ref, w2_ref, w3_ref))
    ]
    for load in loads:
        load.start()
    at_x, core = place_ref[0], place_ref[1]
    rows = send_ref.shape[0]
    deep = attended_ref.shape[2]
    mine = pl.multiple_of(core * rows, CHUNK)
    theirs = pl.multiple_of((1 - core) * rows, CHUNK)
    for j, shift_x in enumerate(SHIFTS):
        source = lax.rem(at_x - shift_x + 4, 4)
        cut = slice(j * deep, (j + 1) * deep)
        rows_ref[:rows, cut] = attended_ref[source, pl.ds(theirs, rows), :]
        rows_ref[rows:, cut] = attended_ref[source, pl.ds(mine, rows), :]
    width = 512
    for half in range(2):
        for load in loads[2 * half : 2 * half + 2]:
            load.wait()
        for n in range(0, send_ref.shape[1], width):
            cut = slice(n, n + width)
            total = 0.0
            for j in (2 * half, 2 * half + 1):
                total = total + dot(rows_ref[:, j * deep : (j + 1) * deep], weights_ref[j, :, cut])
            if half == 0:
                total_ref[:, cut] = total
            else:
                total = total + total_ref[:, cut]
                send_ref[:, cut] = total[:rows].astype(BF16)
                keep_ref[:, cut] = total[rows:]


def final_kernel(latent_ref, keep_ref, got_ref, planes_ref, out_ref):
    gate = row_vector(planes_ref, 4, planes_ref.shape[2] // 5)

    def step(i, carry):
        cut = pl.ds(pl.multiple_of(i * CHUNK, CHUNK), CHUNK)
        mixed = keep_ref[cut, :] + got_ref[cut, :].astype(F32)
        out_ref[cut, :] = (latent_ref[cut, :].astype(F32) + gate * mixed).astype(BF16)
        return carry

    lax.fori_loop(0, latent_ref.shape[0] // CHUNK, step, 0)


def from_other_x(block):
    got = []
    for shift in SHIFTS[1:]:
        got.append(lax.ppermute(block, "x", [(i, (i + shift) % 4) for i in range(4)]))
    return got


def swapped(x):
    return lax.ppermute(x, "c", [(0, 1), (1, 0)])


def tables(first_line, lines):
    inv_freq = 10000.0 ** (-jnp.arange(0, HEAD_DIM // 2, 2, dtype=F32) / (HEAD_DIM // 2))
    at = jnp.concatenate([first_line + jnp.arange(lines), jnp.arange(GRID_W)])
    angles = at.astype(F32)[:, None] * inv_freq
    cosine, sine = jnp.cos(angles), jnp.sin(angles)
    table = jnp.concatenate([cosine, cosine, -sine, sine], axis=1)
    return table[:lines], table[lines:]


def shards(
    latent,
    condition,
    context_condition,
    context,
    norm_gain,
    shift_weight,
    scale_weight,
    gate_weight,
    query_weight,
    key_matrix,
    value_matrix,
    sink_logit_head,
    out_weight,
):
    nz, ny, nx, nc = (lax.axis_size(a) for a in ALL)
    rows, width = latent.shape
    group_rows = rows * nx * nc
    columns = shift_weight.shape[1]
    place = lax.axis_index(SP)
    gain = norm_gain.reshape(1, width)
    parts = pl.pallas_call(
        parts_kernel,
        out_shape=shape_of((nz, 1, 5 * columns), F32),
        in_specs=[VMEM] * 5,
        out_specs=VMEM,
        name="parts",
        compiler_params=vmem(6),
    )(
        *far(condition.reshape(1, -1), context_condition.reshape(1, -1)),
        *far(shift_weight, scale_weight, gate_weight),
    )
    parts = exchanged(parts, "z")
    latent_others = from_other_x(latent)
    lines, cols = tables(place * (group_rows // GRID_W), group_rows // GRID_W)
    count = nz * ny
    where = jnp.stack(
        [
            lax.axis_index("x").astype(jnp.int32),
            lax.axis_index("c").astype(jnp.int32),
            (place == 0).astype(jnp.int32),
            (place == count - 1).astype(jnp.int32),
        ]
    )
    members = ny * nx * nc
    sums = pl.pallas_call(
        sum_kernel,
        out_shape=shape_of((members, 1, 5 * columns), F32),
        in_specs=[VMEM],
        out_specs=VMEM,
        name="sums",
        compiler_params=vmem(4),
    )(*held(parts))
    planes = exchanged(sums, PLANE)
    out_others = from_other_x(out_weight)
    latent_x = jnp.stack([latent, *latent_others])
    latent_c = swapped(latent_x)
    ctx_rows = context.shape[0]
    pairs = pl.pallas_call(
        context_kernel,
        out_shape=shape_of((nz, ctx_rows, 2 * HEAD_DIM), BF16),
        in_specs=[VMEM] * 5,
        out_specs=VMEM,
        name="context_pairs",
        compiler_params=vmem(8),
    )(*far(context), *held(planes), *far(gain, key_matrix, value_matrix))
    ctx_z = exchanged(pairs, "z").reshape(nz * ctx_rows, 2 * HEAD_DIM)
    ctx_pairs = exchanged(copies(ctx_z, "y"), "y").reshape(-1, 2 * HEAD_DIM)
    wide = (group_rows, 2 * HEAD_DIM)
    edge = (WINDOW_REACH, 2 * HEAD_DIM)
    queries, pairs, top, bottom = pl.pallas_call(
        qkv_kernel,
        out_shape=[shape_of(wide, BF16)] * 2 + [pltpu.VMEM(edge, BF16)] * 2,
        in_specs=[SMEM] + [VMEM] * 4 + [HBM] * 3 + [VMEM] * 2,
        out_specs=[VMEM] * 4,
        scratch_shapes=[
            pltpu.VMEM((group_rows, width), BF16),
            pltpu.VMEM((width, 2 * HEAD_DIM), BF16),
            pltpu.VMEM((width, 2 * HEAD_DIM), BF16),
            pltpu.SemaphoreType.DMA((3,)),
        ],
        name="qkv",
        compiler_params=vmem(20),
    )(
        where,
        *held(latent_x, latent_c, planes, gain),
        *far(query_weight, key_matrix, value_matrix),
        *held(lines, cols),
    )
    low = lax.ppermute(bottom, SP, [(i, i + 1) for i in range(count - 1)])
    high = lax.ppermute(top, SP, [(i + 1, i) for i in range(count - 1)])
    long = group_rows + 2 * WINDOW_REACH
    attended = pl.pallas_call(
        attention_kernel,
        out_shape=shape_of(wide, BF16),
        in_specs=[SMEM] * 2 + [VMEM] * 5,
        out_specs=VMEM,
        scratch_shapes=[
            pltpu.VMEM((long, HEAD_DIM), BF16),
            pltpu.VMEM((long, 2 * HEAD_DIM), BF16),
            pltpu.VMEM((count * ctx_rows, 2 * HEAD_DIM), BF16),
        ],
        name="attention",
        compiler_params=vmem(16),
    )(where, sink_logit_head, *held(queries, low, pairs, high, ctx_pairs))
    attended = exchanged(attended.reshape(nx, nc * rows, 2 * HEAD_DIM), "x")
    send, keep = pl.pallas_call(
        project_kernel,
        out_shape=[pltpu.VMEM((rows, width), BF16), pltpu.VMEM((rows, width), F32)],
        in_specs=[SMEM, VMEM] + [HBM] * 4,
        out_specs=(VMEM, VMEM),
        scratch_shapes=[
            pltpu.VMEM((nc * rows, nx * 2 * HEAD_DIM), BF16),
            pltpu.VMEM((nc * rows, width), F32),
            pltpu.VMEM((nx, 2 * HEAD_DIM, width), BF16),
            pltpu.SemaphoreType.DMA((4,)),
        ],
        name="project",
        compiler_params=vmem(14),
    )(where, *held(attended), *far(out_weight, *out_others))
    got = swapped(send)
    return pl.pallas_call(
        final_kernel,
        out_shape=shape_of((rows, width), BF16),
        in_specs=[VMEM] * 4,
        out_specs=VMEM,
        name="final",
        compiler_params=vmem(8),
    )(*far(latent), *held(keep, got, planes))


def solution(mesh):
    torus = Mesh(mesh.devices.reshape(16, 4, 4, 2), ALL)

    return jax.shard_map(
        shards,
        mesh=torus,
        in_specs=(
            P(ALL, None),
            P(SP),
            P(SP),
            P(SP, None),
            P(),
            P(SP, TP),
            P(SP, TP),
            P(SP, TP),
            P(None, TP),
            P(None, TP),
            P(None, TP),
            P(TP),
            P(TP, None),
        ),
        out_specs=P(ALL, None),
        check_vma=False,
    )
```

```python
import jax
import jax.numpy as jnp
from jax import lax
from jax.experimental import pallas as pl
from jax.experimental.pallas import tpu as pltpu
from jax.sharding import Mesh
from jax.sharding import PartitionSpec as P

HEAD_DIM = 128
WINDOW_REACH = 128
GRID_W = 64
SP = ("z", "y")
TP = ("x", "c")
PLANE = ("y", "x", "c")
ALL = ("z", "y", "x", "c")
NORM_EPS = 1e-05
MASKED_SCORE = -1e30
LOG2_E = 1.4426950408889634
CHUNK = 16
SHIFTS = (0, 1, 3, 2)


VMEM = pl.BlockSpec(memory_space=pltpu.VMEM)
SMEM = pl.BlockSpec(memory_space=pltpu.SMEM)
HBM = pl.BlockSpec(memory_space=pltpu.HBM)
F32 = jnp.float32
BF16 = jnp.bfloat16


def shape_of(shape, dtype):
    return jax.ShapeDtypeStruct(shape, dtype)


def vmem(mib):
    return pltpu.CompilerParams(vmem_limit_bytes=mib * 2**20)


def held(*arrays):
    return [pltpu.with_memory_space_constraint(a, pltpu.VMEM) for a in arrays]


def far(*arrays):
    return [pltpu.with_memory_space_constraint(a, pltpu.HBM) for a in arrays]


def exchanged(blocks, axis):
    return lax.all_to_all(blocks, axis, 0, 0, tiled=True)


def dot(a, b):
    return jnp.dot(a, b, preferred_element_type=F32)


def row_vector(planes_ref, index, columns):
    count = planes_ref.shape[0] // 4
    cut = pl.ds(index * columns, columns)
    pieces = []
    for t in range(count):
        piece = planes_ref[t, :, cut]
        for y in range(1, 4):
            piece = piece + planes_ref[y * count + t, :, cut]
        pieces.append(piece)
    return jnp.concatenate(pieces, axis=1)


def parts_kernel(cond_ref, ctx_cond_ref, shift_ref, scale_ref, gate_ref, out_ref):
    def active(ref):
        v = ref[...]
        return (v / (1.0 + jnp.exp(-v))).astype(BF16)

    both = jnp.concatenate([active(cond_ref), active(ctx_cond_ref)], axis=0)
    both = jnp.concatenate([both, jnp.zeros((14, both.shape[1]), BF16)], axis=0)
    shift = dot(both, shift_ref[...])
    scale = dot(both, scale_ref[...])
    gate = dot(both, gate_ref[...])
    row = jnp.concatenate([shift[0:1], shift[1:2], scale[0:1], scale[1:2], gate[0:1]], axis=1)
    for i in range(out_ref.shape[0]):
        out_ref[i] = row


def normed_rows(ref, x, start, multiplier, shift):
    rows = ref[x, pl.ds(start, CHUNK), :].astype(F32)
    mean = jnp.mean(rows * rows, axis=-1, keepdims=True)
    return (rows * lax.rsqrt(mean + NORM_EPS) * multiplier + shift).astype(BF16)


def turned(u, cosine, sine):
    lane = lax.broadcasted_iota(jnp.int32, u.shape, 1)
    first = (lane % 64) < 32
    swapped = jnp.where(first, pltpu.roll(u, 96, 1), pltpu.roll(u, 32, 1))
    return u * cosine + swapped * sine


def sum_kernel(parts_ref, out_ref):
    total = parts_ref[0]
    for z in range(1, parts_ref.shape[0]):
        total = total + parts_ref[z]
    for p in range(out_ref.shape[0]):
        out_ref[p] = total


def qkv_kernel(
    place_ref, own_ref, other_ref, planes_ref, gain_ref, wq_ref, wk_ref, wv_ref, row_ref, col_ref,
    q_ref, kv_ref, top_ref, bottom_ref, hidden_ref, wq_held_ref, wkv_ref, sems,
):
    columns = wq_ref.shape[1]
    loads = (
        pltpu.make_async_copy(wq_ref, wq_held_ref, sems.at[0]),
        pltpu.make_async_copy(wk_ref, wkv_ref.at[:, :HEAD_DIM], sems.at[1]),
        pltpu.make_async_copy(wv_ref, wkv_ref.at[:, HEAD_DIM:], sems.at[2]),
    )
    for load in loads:
        load.start()
    shift = row_vector(planes_ref, 0, columns)
    multiplier = gain_ref[...] * (1.0 + row_vector(planes_ref, 2, columns))
    _, rows, _ = own_ref.shape
    at_x, core = place_ref[0], place_ref[1]
    for x, shift_x in enumerate(SHIFTS):
        source = lax.rem(at_x - shift_x + 4, 4)
        mine = (2 * source + core) * rows
        theirs = (2 * source + 1 - core) * rows

        def step(i, carry, x=x, mine=mine, theirs=theirs):
            start = pl.multiple_of(i * CHUNK, CHUNK)
            at = pl.multiple_of(mine + start, CHUNK)
            hidden_ref[pl.ds(at, CHUNK), :] = normed_rows(own_ref, x, start, multiplier, shift)
            at = pl.multiple_of(theirs + start, CHUNK)
            hidden_ref[pl.ds(at, CHUNK), :] = normed_rows(other_ref, x, start, multiplier, shift)
            return carry

        lax.fori_loop(0, rows // CHUNK, step, 0, unroll=2)
    for load in loads:
        load.wait()
    block = 384
    lane = lax.broadcasted_iota(jnp.int32, (GRID_W, HEAD_DIM), 1) < 64
    col = col_ref[...]
    col_turned = pltpu.roll(col, 64, 1)
    row_turned = pltpu.roll(row_ref[...], 64, 1)
    factor = HEAD_DIM ** (-0.5) * LOG2_E
    for at in range(0, hidden_ref.shape[0], block):
        cut = slice(at, at + block)
        hidden = hidden_ref[cut, :]
        lines = range(at // GRID_W, (at + block) // GRID_W)
        cosine = jnp.concatenate(
            [jnp.where(lane, row_ref[g : g + 1, :], col_turned) for g in lines], axis=0
        )
        sine = jnp.concatenate(
            [jnp.where(lane, row_turned[g : g + 1, :], col) for g in lines], axis=0
        )
        queries = dot(hidden, wq_held_ref[...])
        for h in range(2):
            part = slice(h * HEAD_DIM, (h + 1) * HEAD_DIM)
            q_ref[cut, part] = (turned(queries[:, part], cosine, sine) * factor).astype(BF16)
        pairs = dot(hidden, wkv_ref[...])
        kv_ref[cut, :HEAD_DIM] = turned(pairs[:, :HEAD_DIM], cosine, sine).astype(BF16)
        kv_ref[cut, HEAD_DIM:] = pairs[:, HEAD_DIM:].astype(BF16)
    top_ref[...] = kv_ref[:WINDOW_REACH, :]
    bottom_ref[...] = kv_ref[hidden_ref.shape[0] - WINDOW_REACH :, :]


def context_kernel(ctx_ref, planes_ref, gain_ref, wk_ref, wv_ref, out_ref):
    columns = planes_ref.shape[2] // 5
    shift = row_vector(planes_ref, 1, columns)
    multiplier = gain_ref[...] * (1.0 + row_vector(planes_ref, 3, columns))
    rows = ctx_ref[...].astype(F32)
    mean = jnp.mean(rows * rows, axis=-1, keepdims=True)
    hidden = (rows * lax.rsqrt(mean + NORM_EPS) * multiplier + shift).astype(BF16)
    pairs = jnp.concatenate([dot(hidden, wk_ref[...]), dot(hidden, wv_ref[...])], axis=1)
    pairs = pairs.astype(BF16)
    for p in range(out_ref.shape[0]):
        out_ref[p] = pairs


def spread_kernel(block_ref, out_ref, sems):
    sends = [
        pltpu.make_async_copy(block_ref, out_ref.at[y], sems.at[y])
        for y in range(out_ref.shape[0])
    ]
    for send in sends:
        send.start()
    for send in sends:
        send.wait()


def attention_kernel(
    place_ref, sink_ref, q_ref, low_ref, kv_ref, high_ref, ctx_ref, attended_ref,
    keys_ref, values_ref, ctx_values_ref,
):
    reach = WINDOW_REACH
    total = kv_ref.shape[0]
    first, last = place_ref[2], place_ref[3]
    for ref, at in ((low_ref, 0), (kv_ref, reach), (high_ref, reach + total)):
        cut = slice(at, at + ref.shape[0])
        keys_ref[cut, :] = ref[:, :HEAD_DIM]
        values_ref[cut, :HEAD_DIM] = ref[:, HEAD_DIM:]
    values_ref[:, HEAD_DIM:] = jnp.ones(keys_ref.shape, BF16)
    ctx_values_ref[:, :HEAD_DIM] = ctx_ref[:, HEAD_DIM:]
    ctx_values_ref[:, HEAD_DIM:] = jnp.ones((ctx_ref.shape[0], HEAD_DIM), BF16)
    row = lax.broadcasted_iota(jnp.int32, (2 * reach, 1), 0)
    sink = jnp.where(row < reach, sink_ref[0], sink_ref[1]) * LOG2_E
    position = lax.broadcasted_iota(jnp.int32, (2 * reach, 3 * reach), 0) % reach
    column = lax.broadcasted_iota(jnp.int32, (2 * reach, 3 * reach), 1)
    band = (column >= position) & (column <= position + 2 * reach)
    blocks = total // reach
    contract = (((1,), (1,)), ((), ()))

    def step(b, carry):
        at = pl.multiple_of(b * reach, reach)
        both = q_ref[pl.ds(at, reach), :]
        queries = jnp.concatenate([both[:, :HEAD_DIM], both[:, HEAD_DIM:]], axis=0)
        keys = keys_ref[pl.ds(at, 3 * reach), :]
        values = values_ref[pl.ds(at, 3 * reach), :]
        lowest = jnp.where(b == 0, first * reach, 0)
        highest = jnp.where(b == blocks - 1, (3 - last) * reach, 3 * reach)
        allowed = band & (column >= lowest) & (column < highest)
        near = lax.dot_general(queries, keys, contract, preferred_element_type=F32)
        near = jnp.where(allowed, near, MASKED_SCORE)
        far = lax.dot_general(
            queries, ctx_ref[:, :HEAD_DIM], contract, preferred_element_type=F32
        )
        top = jnp.maximum(
            jnp.max(near, axis=-1, keepdims=True), jnp.max(far, axis=-1, keepdims=True)
        )
        top = jnp.maximum(top, sink)
        near = jnp.exp2(near - top).astype(BF16)
        far = jnp.exp2(far - top).astype(BF16)
        mixed = dot(near, values) + dot(far, ctx_values_ref[...])
        share = mixed[:, HEAD_DIM:] + jnp.exp2(sink - top)
        mixed = (mixed[:, :HEAD_DIM] / share).astype(BF16)
        attended_ref[pl.ds(at, reach), :HEAD_DIM] = mixed[:reach]
        attended_ref[pl.ds(at, reach), HEAD_DIM:] = mixed[reach:]
        return carry

    lax.fori_loop(0, blocks, step, 0, unroll=2)


def project_kernel(
    place_ref, attended_ref, w0_ref, w1_ref, w2_ref, w3_ref, send_ref, keep_ref,
    rows_ref, weights_ref, sems,
):
    width = 512
    cuts = [slice(n, n + width) for n in range(0, send_ref.shape[1], width)]
    loads = [
        [
            pltpu.make_async_copy(w.at[:, cut], weights_ref.at[j, :, cut], sems.at[n, j])
            for j, w in enumerate((w0_ref, w1_ref, w2_ref, w3_ref))
        ]
        for n, cut in enumerate(cuts)
    ]
    for group in loads:
        for load in group:
            load.start()
    at_x, core = place_ref[0], place_ref[1]
    rows = send_ref.shape[0]
    deep = attended_ref.shape[2]
    mine = pl.multiple_of(core * rows, CHUNK)
    theirs = pl.multiple_of((1 - core) * rows, CHUNK)
    for j, shift_x in enumerate(SHIFTS):
        source = lax.rem(at_x - shift_x + 4, 4)
        cut = slice(j * deep, (j + 1) * deep)
        rows_ref[:rows, cut] = attended_ref[source, pl.ds(theirs, rows), :]
        rows_ref[rows:, cut] = attended_ref[source, pl.ds(mine, rows), :]
    for group, cut in zip(loads, cuts):
        for load in group:
            load.wait()
        total = dot(rows_ref[:, :deep], weights_ref[0, :, cut])
        for j in range(1, 4):
            total = total + dot(rows_ref[:, j * deep : (j + 1) * deep], weights_ref[j, :, cut])
        send_ref[:, cut] = total[:rows].astype(BF16)
        keep_ref[:, cut] = total[rows:]


def final_kernel(latent_ref, keep_ref, got_ref, planes_ref, out_ref):
    gate = row_vector(planes_ref, 4, planes_ref.shape[2] // 5)

    def step(i, carry):
        cut = pl.ds(pl.multiple_of(i * CHUNK, CHUNK), CHUNK)
        mixed = keep_ref[cut, :] + got_ref[cut, :].astype(F32)
        out_ref[cut, :] = (latent_ref[cut, :].astype(F32) + gate * mixed).astype(BF16)
        return carry

    lax.fori_loop(0, latent_ref.shape[0] // CHUNK, step, 0)


def from_other_x(block):
    got = []
    for shift in SHIFTS[1:]:
        got.append(lax.ppermute(block, "x", [(i, (i + shift) % 4) for i in range(4)]))
    return got


def swapped(x):
    return lax.ppermute(x, "c", [(0, 1), (1, 0)])


def tables(first_line, lines):
    inv_freq = 10000.0 ** (-jnp.arange(0, HEAD_DIM // 2, 2, dtype=F32) / (HEAD_DIM // 2))
    at = jnp.concatenate([first_line + jnp.arange(lines), jnp.arange(GRID_W)])
    angles = at.astype(F32)[:, None] * inv_freq
    cosine, sine = jnp.cos(angles), jnp.sin(angles)
    table = jnp.concatenate([cosine, cosine, -sine, sine], axis=1)
    return table[:lines], table[lines:]


def shards(
    latent,
    condition,
    context_condition,
    context,
    norm_gain,
    shift_weight,
    scale_weight,
    gate_weight,
    query_weight,
    key_matrix,
    value_matrix,
    sink_logit_head,
    out_weight,
):
    nz, ny, nx, nc = (lax.axis_size(a) for a in ALL)
    rows, width = latent.shape
    group_rows = rows * nx * nc
    columns = shift_weight.shape[1]
    place = lax.axis_index(SP)
    gain = norm_gain.reshape(1, width)
    parts = pl.pallas_call(
        parts_kernel,
        out_shape=shape_of((nz, 1, 5 * columns), F32),
        in_specs=[VMEM] * 5,
        out_specs=VMEM,
        name="parts",
        compiler_params=vmem(6),
    )(
        *far(condition.reshape(1, -1), context_condition.reshape(1, -1)),
        *far(shift_weight, scale_weight, gate_weight),
    )
    parts = exchanged(parts, "z")
    latent_others = from_other_x(latent)
    lines, cols = tables(place * (group_rows // GRID_W), group_rows // GRID_W)
    count = nz * ny
    where = jnp.stack(
        [
            lax.axis_index("x").astype(jnp.int32),
            lax.axis_index("c").astype(jnp.int32),
            (place == 0).astype(jnp.int32),
            (place == count - 1).astype(jnp.int32),
        ]
    )
    members = ny * nx * nc
    sums = pl.pallas_call(
        sum_kernel,
        out_shape=shape_of((members, 1, 5 * columns), F32),
        in_specs=[VMEM],
        out_specs=VMEM,
        name="sums",
        compiler_params=vmem(4),
    )(*held(parts))
    planes = exchanged(sums, PLANE)
    out_others = from_other_x(out_weight)
    latent_x = jnp.stack([latent, *latent_others])
    latent_c = swapped(latent_x)
    ctx_rows = context.shape[0]
    pairs = pl.pallas_call(
        context_kernel,
        out_shape=shape_of((nz, ctx_rows, 2 * HEAD_DIM), BF16),
        in_specs=[VMEM] * 5,
        out_specs=VMEM,
        name="context_pairs",
        compiler_params=vmem(8),
    )(*held(context, planes, gain, key_matrix, value_matrix))
    ctx_z = exchanged(pairs, "z").reshape(nz * ctx_rows, 2 * HEAD_DIM)
    spread = pl.pallas_call(
        spread_kernel,
        out_shape=pltpu.HBM((ny, *ctx_z.shape), BF16),
        in_specs=[VMEM],
        out_specs=HBM,
        scratch_shapes=[pltpu.SemaphoreType.DMA((ny,))],
        name="spread",
        compiler_params=vmem(4),
    )(*held(ctx_z))
    ctx_pairs = exchanged(spread, "y").reshape(-1, 2 * HEAD_DIM)
    wide = (group_rows, 2 * HEAD_DIM)
    edge = (WINDOW_REACH, 2 * HEAD_DIM)
    queries, pairs, top, bottom = pl.pallas_call(
        qkv_kernel,
        out_shape=[pltpu.HBM(wide, BF16)] * 2 + [pltpu.VMEM(edge, BF16)] * 2,
        in_specs=[SMEM] + [VMEM] * 4 + [HBM] * 3 + [VMEM] * 2,
        out_specs=[VMEM] * 4,
        scratch_shapes=[
            pltpu.VMEM((group_rows, width), BF16),
            pltpu.VMEM((width, 2 * HEAD_DIM), BF16),
            pltpu.VMEM((width, 2 * HEAD_DIM), BF16),
            pltpu.SemaphoreType.DMA((3,)),
        ],
        name="qkv",
        compiler_params=vmem(20),
    )(
        where,
        *held(latent_x, latent_c, planes, gain),
        *far(query_weight, key_matrix, value_matrix),
        *held(lines, cols),
    )
    low = lax.ppermute(bottom, SP, [(i, i + 1) for i in range(count - 1)])
    high = lax.ppermute(top, SP, [(i + 1, i) for i in range(count - 1)])
    long = group_rows + 2 * WINDOW_REACH
    attended = pl.pallas_call(
        attention_kernel,
        out_shape=shape_of(wide, BF16),
        in_specs=[SMEM] * 2 + [VMEM] * 5,
        out_specs=VMEM,
        scratch_shapes=[
            pltpu.VMEM((long, HEAD_DIM), BF16),
            pltpu.VMEM((long, 2 * HEAD_DIM), BF16),
            pltpu.VMEM((count * ctx_rows, 2 * HEAD_DIM), BF16),
        ],
        name="attention",
        compiler_params=vmem(16),
    )(where, sink_logit_head, *held(queries, low, pairs, high, ctx_pairs))
    attended = exchanged(attended.reshape(nx, nc * rows, 2 * HEAD_DIM), "x")
    send, keep = pl.pallas_call(
        project_kernel,
        out_shape=[pltpu.VMEM((rows, width), BF16), pltpu.VMEM((rows, width), F32)],
        in_specs=[SMEM, VMEM] + [HBM] * 4,
        out_specs=(VMEM, VMEM),
        scratch_shapes=[
            pltpu.VMEM((nc * rows, nx * 2 * HEAD_DIM), BF16),
            pltpu.VMEM((nx, 2 * HEAD_DIM, width), BF16),
            pltpu.SemaphoreType.DMA((4, 4)),
        ],
        name="project",
        compiler_params=vmem(14),
    )(where, *held(attended), *far(out_weight, *out_others))
    got = swapped(send)
    return pl.pallas_call(
        final_kernel,
        out_shape=shape_of((rows, width), BF16),
        in_specs=[VMEM] * 4,
        out_specs=VMEM,
        name="final",
        compiler_params=vmem(8),
    )(*held(latent, keep, got, planes))


def solution(mesh):
    torus = Mesh(mesh.devices.reshape(16, 4, 4, 2), ALL)

    return jax.shard_map(
        shards,
        mesh=torus,
        in_specs=(
            P(ALL, None),
            P(SP),
            P(SP),
            P(SP, None),
            P(),
            P(SP, TP),
            P(SP, TP),
            P(SP, TP),
            P(None, TP),
            P(None, TP),
            P(None, TP),
            P(TP),
            P(TP, None),
        ),
        out_specs=P(ALL, None),
        check_vma=False,
    )
```

```python
import jax
import jax.numpy as jnp
from jax import lax
from jax.experimental import pallas as pl
from jax.experimental.pallas import tpu as pltpu
from jax.sharding import Mesh
from jax.sharding import PartitionSpec as P

HEAD_DIM = 128
WINDOW_REACH = 128
GRID_W = 64
SP = ("z", "y")
TP = ("x", "c")
PLANE = ("y", "x", "c")
ALL = ("z", "y", "x", "c")
NORM_EPS = 1e-05
MASKED_SCORE = -1e30
LOG2_E = 1.4426950408889634
CHUNK = 16
SHIFTS = (0, 1, 3, 2)


VMEM = pl.BlockSpec(memory_space=pltpu.VMEM)
SMEM = pl.BlockSpec(memory_space=pltpu.SMEM)
HBM = pl.BlockSpec(memory_space=pltpu.HBM)
F32 = jnp.float32
BF16 = jnp.bfloat16


def shape_of(shape, dtype):
    return jax.ShapeDtypeStruct(shape, dtype)


def vmem(mib):
    return pltpu.CompilerParams(vmem_limit_bytes=mib * 2**20)


def held(*arrays):
    return [pltpu.with_memory_space_constraint(a, pltpu.VMEM) for a in arrays]


def far(*arrays):
    return [pltpu.with_memory_space_constraint(a, pltpu.HBM) for a in arrays]


def exchanged(blocks, axis):
    return lax.all_to_all(blocks, axis, 0, 0, tiled=True)


def dot(a, b):
    return jnp.dot(a, b, preferred_element_type=F32)


def row_vector(planes_ref, index, columns):
    count = planes_ref.shape[0] // 4
    cut = pl.ds(index * columns, columns)
    pieces = []
    for t in range(count):
        piece = planes_ref[t, :, cut]
        for y in range(1, 4):
            piece = piece + planes_ref[y * count + t, :, cut]
        pieces.append(piece)
    return jnp.concatenate(pieces, axis=1)


def parts_kernel(cond_ref, ctx_cond_ref, shift_ref, scale_ref, gate_ref, out_ref):
    def active(ref):
        v = ref[...]
        return (v / (1.0 + jnp.exp(-v))).astype(BF16)

    both = jnp.concatenate([active(cond_ref), active(ctx_cond_ref)], axis=0)
    both = jnp.concatenate([both, jnp.zeros((14, both.shape[1]), BF16)], axis=0)
    shift = dot(both, shift_ref[...])
    scale = dot(both, scale_ref[...])
    gate = dot(both, gate_ref[...])
    row = jnp.concatenate([shift[0:1], shift[1:2], scale[0:1], scale[1:2], gate[0:1]], axis=1)
    for i in range(out_ref.shape[0]):
        out_ref[i] = row


def normed_rows(ref, x, start, multiplier, shift):
    rows = ref[x, pl.ds(start, CHUNK), :].astype(F32)
    mean = jnp.mean(rows * rows, axis=-1, keepdims=True)
    return (rows * lax.rsqrt(mean + NORM_EPS) * multiplier + shift).astype(BF16)


def turned(u, cosine, sine):
    lane = lax.broadcasted_iota(jnp.int32, u.shape, 1)
    first = (lane % 64) < 32
    swapped = jnp.where(first, pltpu.roll(u, 96, 1), pltpu.roll(u, 32, 1))
    return u * cosine + swapped * sine


def sum_kernel(parts_ref, out_ref):
    total = parts_ref[0]
    for z in range(1, parts_ref.shape[0]):
        total = total + parts_ref[z]
    for p in range(out_ref.shape[0]):
        out_ref[p] = total


def qkv_kernel(
    place_ref, own_ref, other_ref, planes_ref, gain_ref, wq_ref, wk_ref, wv_ref, row_ref, col_ref,
    q_ref, kv_ref, top_ref, bottom_ref, hidden_ref, wq_held_ref, wkv_ref, sems,
):
    columns = wq_ref.shape[1]
    loads = (
        pltpu.make_async_copy(wq_ref, wq_held_ref, sems.at[0]),
        pltpu.make_async_copy(wk_ref, wkv_ref.at[:, :HEAD_DIM], sems.at[1]),
        pltpu.make_async_copy(wv_ref, wkv_ref.at[:, HEAD_DIM:], sems.at[2]),
    )
    for load in loads:
        load.start()
    shift = row_vector(planes_ref, 0, columns)
    multiplier = gain_ref[...] * (1.0 + row_vector(planes_ref, 2, columns))
    _, rows, _ = own_ref.shape
    at_x, core = place_ref[0], place_ref[1]
    for x, shift_x in enumerate(SHIFTS):
        source = lax.rem(at_x - shift_x + 4, 4)
        mine = (2 * source + core) * rows
        theirs = (2 * source + 1 - core) * rows

        def step(i, carry, x=x, mine=mine, theirs=theirs):
            start = pl.multiple_of(i * CHUNK, CHUNK)
            at = pl.multiple_of(mine + start, CHUNK)
            hidden_ref[pl.ds(at, CHUNK), :] = normed_rows(own_ref, x, start, multiplier, shift)
            at = pl.multiple_of(theirs + start, CHUNK)
            hidden_ref[pl.ds(at, CHUNK), :] = normed_rows(other_ref, x, start, multiplier, shift)
            return carry

        lax.fori_loop(0, rows // CHUNK, step, 0, unroll=2)
    for load in loads:
        load.wait()
    block = 384
    lane = lax.broadcasted_iota(jnp.int32, (GRID_W, HEAD_DIM), 1) < 64
    col = col_ref[...]
    col_turned = pltpu.roll(col, 64, 1)
    row_turned = pltpu.roll(row_ref[...], 64, 1)
    factor = HEAD_DIM ** (-0.5) * LOG2_E
    for at in range(0, hidden_ref.shape[0], block):
        cut = slice(at, at + block)
        hidden = hidden_ref[cut, :]
        lines = range(at // GRID_W, (at + block) // GRID_W)
        cosine = jnp.concatenate(
            [jnp.where(lane, row_ref[g : g + 1, :], col_turned) for g in lines], axis=0
        )
        sine = jnp.concatenate(
            [jnp.where(lane, row_turned[g : g + 1, :], col) for g in lines], axis=0
        )
        queries = dot(hidden, wq_held_ref[...])
        for h in range(2):
            part = slice(h * HEAD_DIM, (h + 1) * HEAD_DIM)
            q_ref[cut, part] = (turned(queries[:, part], cosine, sine) * factor).astype(BF16)
        pairs = dot(hidden, wkv_ref[...])
        kv_ref[cut, :HEAD_DIM] = turned(pairs[:, :HEAD_DIM], cosine, sine).astype(BF16)
        kv_ref[cut, HEAD_DIM:] = pairs[:, HEAD_DIM:].astype(BF16)
    top_ref[...] = kv_ref[:WINDOW_REACH, :]
    bottom_ref[...] = kv_ref[hidden_ref.shape[0] - WINDOW_REACH :, :]


def context_kernel(
    ctx_ref, planes_ref, gain_ref, wk_ref, wv_ref, out_ref, wkv_ref, sems
):
    loads = (
        pltpu.make_async_copy(wk_ref, wkv_ref.at[:, :HEAD_DIM], sems.at[0]),
        pltpu.make_async_copy(wv_ref, wkv_ref.at[:, HEAD_DIM:], sems.at[1]),
    )
    for load in loads:
        load.start()
    columns = planes_ref.shape[2] // 5
    shift = row_vector(planes_ref, 1, columns)
    multiplier = gain_ref[...] * (1.0 + row_vector(planes_ref, 3, columns))
    rows = ctx_ref[...].astype(F32)
    mean = jnp.mean(rows * rows, axis=-1, keepdims=True)
    hidden = (rows * lax.rsqrt(mean + NORM_EPS) * multiplier + shift).astype(BF16)
    for load in loads:
        load.wait()
    pairs = dot(hidden, wkv_ref[...]).astype(BF16)
    for p in range(out_ref.shape[0]):
        out_ref[p] = pairs


def spread_kernel(block_ref, out_ref, sems):
    sends = [
        pltpu.make_async_copy(block_ref, out_ref.at[y], sems.at[y])
        for y in range(out_ref.shape[0])
    ]
    for send in sends:
        send.start()
    for send in sends:
        send.wait()


def attention_kernel(
    place_ref, sink_ref, q_ref, low_ref, kv_ref, high_ref, ctx_ref, attended_ref,
    keys_ref, values_ref, ctx_values_ref,
):
    reach = WINDOW_REACH
    total = kv_ref.shape[0]
    first, last = place_ref[2], place_ref[3]
    for ref, at in ((low_ref, 0), (kv_ref, reach), (high_ref, reach + total)):
        cut = slice(at, at + ref.shape[0])
        keys_ref[cut, :] = ref[:, :HEAD_DIM]
        values_ref[cut, :HEAD_DIM] = ref[:, HEAD_DIM:]
    values_ref[:, HEAD_DIM:] = jnp.ones(keys_ref.shape, BF16)
    ctx_values_ref[:, :HEAD_DIM] = ctx_ref[:, HEAD_DIM:]
    ctx_values_ref[:, HEAD_DIM:] = jnp.ones((ctx_ref.shape[0], HEAD_DIM), BF16)
    row = lax.broadcasted_iota(jnp.int32, (2 * reach, 1), 0)
    sink = jnp.where(row < reach, sink_ref[0], sink_ref[1]) * LOG2_E
    position = lax.broadcasted_iota(jnp.int32, (2 * reach, 3 * reach), 0) % reach
    column = lax.broadcasted_iota(jnp.int32, (2 * reach, 3 * reach), 1)
    band = (column >= position) & (column <= position + 2 * reach)
    blocks = total // reach
    contract = (((1,), (1,)), ((), ()))

    def step(b, carry):
        at = pl.multiple_of(b * reach, reach)
        both = q_ref[pl.ds(at, reach), :]
        queries = jnp.concatenate([both[:, :HEAD_DIM], both[:, HEAD_DIM:]], axis=0)
        keys = keys_ref[pl.ds(at, 3 * reach), :]
        values = values_ref[pl.ds(at, 3 * reach), :]
        lowest = jnp.where(b == 0, first * reach, 0)
        highest = jnp.where(b == blocks - 1, (3 - last) * reach, 3 * reach)
        allowed = band & (column >= lowest) & (column < highest)
        near = lax.dot_general(queries, keys, contract, preferred_element_type=F32)
        near = jnp.where(allowed, near, MASKED_SCORE)
        far = lax.dot_general(
            queries, ctx_ref[:, :HEAD_DIM], contract, preferred_element_type=F32
        )
        top = jnp.maximum(
            jnp.max(near, axis=-1, keepdims=True), jnp.max(far, axis=-1, keepdims=True)
        )
        top = jnp.maximum(top, sink)
        near = jnp.exp2(near - top).astype(BF16)
        far = jnp.exp2(far - top).astype(BF16)
        mixed = dot(near, values) + dot(far, ctx_values_ref[...])
        share = mixed[:, HEAD_DIM:] + jnp.exp2(sink - top)
        mixed = (mixed[:, :HEAD_DIM] / share).astype(BF16)
        attended_ref[pl.ds(at, reach), :HEAD_DIM] = mixed[:reach]
        attended_ref[pl.ds(at, reach), HEAD_DIM:] = mixed[reach:]
        return carry

    lax.fori_loop(0, blocks, step, 0, unroll=2)


def load_kernel(w0_ref, w1_ref, out_ref, sems):
    loads = [
        pltpu.make_async_copy(w, out_ref.at[j], sems.at[j])
        for j, w in enumerate((w0_ref, w1_ref))
    ]
    for load in loads:
        load.start()
    for load in loads:
        load.wait()


def project_kernel(
    place_ref, attended_ref, early_ref, w2_ref, w3_ref, send_ref, keep_ref,
    rows_ref, late_ref, sems,
):
    width = 512
    cuts = [slice(n, n + width) for n in range(0, send_ref.shape[1], width)]
    loads = [
        [
            pltpu.make_async_copy(w.at[:, cut], late_ref.at[j, :, cut], sems.at[n, j])
            for j, w in enumerate((w2_ref, w3_ref))
        ]
        for n, cut in enumerate(cuts)
    ]
    for group in loads:
        for load in group:
            load.start()
    at_x, core = place_ref[0], place_ref[1]
    rows = send_ref.shape[0]
    deep = attended_ref.shape[2]
    mine = pl.multiple_of(core * rows, CHUNK)
    theirs = pl.multiple_of((1 - core) * rows, CHUNK)
    for j, shift_x in enumerate(SHIFTS):
        source = lax.rem(at_x - shift_x + 4, 4)
        cut = slice(j * deep, (j + 1) * deep)
        rows_ref[:rows, cut] = attended_ref[source, pl.ds(theirs, rows), :]
        rows_ref[rows:, cut] = attended_ref[source, pl.ds(mine, rows), :]
    for group, cut in zip(loads, cuts):
        total = dot(rows_ref[:, :deep], early_ref[0, :, cut])
        total = total + dot(rows_ref[:, deep : 2 * deep], early_ref[1, :, cut])
        for load in group:
            load.wait()
        for j in range(2):
            part = slice((2 + j) * deep, (3 + j) * deep)
            total = total + dot(rows_ref[:, part], late_ref[j, :, cut])
        send_ref[:, cut] = total[:rows].astype(BF16)
        keep_ref[:, cut] = total[rows:]


def final_kernel(latent_ref, keep_ref, got_ref, planes_ref, out_ref):
    gate = row_vector(planes_ref, 4, planes_ref.shape[2] // 5)

    def step(i, carry):
        cut = pl.ds(pl.multiple_of(i * CHUNK, CHUNK), CHUNK)
        mixed = keep_ref[cut, :] + got_ref[cut, :].astype(F32)
        out_ref[cut, :] = (latent_ref[cut, :].astype(F32) + gate * mixed).astype(BF16)
        return carry

    lax.fori_loop(0, latent_ref.shape[0] // CHUNK, step, 0)


def from_other_x(block):
    got = []
    for shift in SHIFTS[1:]:
        got.append(lax.ppermute(block, "x", [(i, (i + shift) % 4) for i in range(4)]))
    return got


def swapped(x):
    return lax.ppermute(x, "c", [(0, 1), (1, 0)])


def tables(first_line, lines):
    inv_freq = 10000.0 ** (-jnp.arange(0, HEAD_DIM // 2, 2, dtype=F32) / (HEAD_DIM // 2))
    at = jnp.concatenate([first_line + jnp.arange(lines), jnp.arange(GRID_W)])
    angles = at.astype(F32)[:, None] * inv_freq
    cosine, sine = jnp.cos(angles), jnp.sin(angles)
    table = jnp.concatenate([cosine, cosine, -sine, sine], axis=1)
    return table[:lines], table[lines:]


def shards(
    latent,
    condition,
    context_condition,
    context,
    norm_gain,
    shift_weight,
    scale_weight,
    gate_weight,
    query_weight,
    key_matrix,
    value_matrix,
    sink_logit_head,
    out_weight,
):
    nz, ny, nx, nc = (lax.axis_size(a) for a in ALL)
    rows, width = latent.shape
    group_rows = rows * nx * nc
    columns = shift_weight.shape[1]
    place = lax.axis_index(SP)
    gain = norm_gain.reshape(1, width)
    parts = pl.pallas_call(
        parts_kernel,
        out_shape=shape_of((nz, 1, 5 * columns), F32),
        in_specs=[VMEM] * 5,
        out_specs=VMEM,
        name="parts",
        compiler_params=vmem(6),
    )(
        *far(condition.reshape(1, -1), context_condition.reshape(1, -1)),
        *far(shift_weight, scale_weight, gate_weight),
    )
    parts = exchanged(parts, "z")
    latent_others = from_other_x(latent)
    lines, cols = tables(place * (group_rows // GRID_W), group_rows // GRID_W)
    count = nz * ny
    where = jnp.stack(
        [
            lax.axis_index("x").astype(jnp.int32),
            lax.axis_index("c").astype(jnp.int32),
            (place == 0).astype(jnp.int32),
            (place == count - 1).astype(jnp.int32),
        ]
    )
    members = ny * nx * nc
    sums = pl.pallas_call(
        sum_kernel,
        out_shape=shape_of((members, 1, 5 * columns), F32),
        in_specs=[VMEM],
        out_specs=VMEM,
        name="sums",
        compiler_params=vmem(4),
    )(*held(parts))
    planes = exchanged(sums, PLANE)
    out_others = from_other_x(out_weight)
    latent_x = jnp.stack([latent, *latent_others])
    latent_c = swapped(latent_x)
    ctx_rows = context.shape[0]
    pairs = pl.pallas_call(
        context_kernel,
        out_shape=shape_of((nz, ctx_rows, 2 * HEAD_DIM), BF16),
        in_specs=[VMEM] * 3 + [HBM] * 2,
        out_specs=VMEM,
        scratch_shapes=[
            pltpu.VMEM((width, 2 * HEAD_DIM), BF16),
            pltpu.SemaphoreType.DMA((2,)),
        ],
        name="context_pairs",
        compiler_params=vmem(8),
    )(*far(context), *held(planes), *far(gain, key_matrix, value_matrix))
    ctx_z = exchanged(pairs, "z").reshape(nz * ctx_rows, 2 * HEAD_DIM)
    spread = pl.pallas_call(
        spread_kernel,
        out_shape=pltpu.HBM((ny, *ctx_z.shape), BF16),
        in_specs=[VMEM],
        out_specs=HBM,
        scratch_shapes=[pltpu.SemaphoreType.DMA((ny,))],
        name="spread",
        compiler_params=vmem(4),
    )(*held(ctx_z))
    ctx_pairs = exchanged(spread, "y").reshape(-1, 2 * HEAD_DIM)
    wide = (group_rows, 2 * HEAD_DIM)
    edge = (WINDOW_REACH, 2 * HEAD_DIM)
    queries, pairs, top, bottom = pl.pallas_call(
        qkv_kernel,
        out_shape=[pltpu.HBM(wide, BF16)] * 2 + [pltpu.VMEM(edge, BF16)] * 2,
        in_specs=[SMEM] + [VMEM] * 4 + [HBM] * 3 + [VMEM] * 2,
        out_specs=[VMEM] * 4,
        scratch_shapes=[
            pltpu.VMEM((group_rows, width), BF16),
            pltpu.VMEM((width, 2 * HEAD_DIM), BF16),
            pltpu.VMEM((width, 2 * HEAD_DIM), BF16),
            pltpu.SemaphoreType.DMA((3,)),
        ],
        name="qkv",
        compiler_params=vmem(20),
    )(
        where,
        *held(latent_x, latent_c, planes, gain),
        *far(query_weight, key_matrix, value_matrix),
        *held(lines, cols),
    )
    low = lax.ppermute(bottom, SP, [(i, i + 1) for i in range(count - 1)])
    high = lax.ppermute(top, SP, [(i + 1, i) for i in range(count - 1)])
    long = group_rows + 2 * WINDOW_REACH
    attended = pl.pallas_call(
        attention_kernel,
        out_shape=shape_of(wide, BF16),
        in_specs=[SMEM] * 2 + [VMEM] * 5,
        out_specs=VMEM,
        scratch_shapes=[
            pltpu.VMEM((long, HEAD_DIM), BF16),
            pltpu.VMEM((long, 2 * HEAD_DIM), BF16),
            pltpu.VMEM((count * ctx_rows, 2 * HEAD_DIM), BF16),
        ],
        name="attention",
        compiler_params=vmem(16),
    )(where, sink_logit_head, *held(queries, low, pairs, high, ctx_pairs))
    attended = exchanged(attended.reshape(nx, nc * rows, 2 * HEAD_DIM), "x")
    weights = pl.pallas_call(
        load_kernel,
        out_shape=pltpu.VMEM((2, *out_weight.shape), BF16),
        in_specs=[HBM] * 2,
        out_specs=VMEM,
        scratch_shapes=[pltpu.SemaphoreType.DMA((2,))],
        name="load",
        compiler_params=vmem(2),
    )(*far(out_weight, out_others[0]))
    send, keep = pl.pallas_call(
        project_kernel,
        out_shape=[pltpu.VMEM((rows, width), BF16), pltpu.VMEM((rows, width), F32)],
        in_specs=[SMEM, VMEM, VMEM, HBM, HBM],
        out_specs=(VMEM, VMEM),
        scratch_shapes=[
            pltpu.VMEM((nc * rows, nx * 2 * HEAD_DIM), BF16),
            pltpu.VMEM((2, 2 * HEAD_DIM, width), BF16),
            pltpu.SemaphoreType.DMA((4, 2)),
        ],
        name="project",
        compiler_params=vmem(14),
    )(where, *held(attended, weights), *far(*out_others[1:]))
    got = swapped(send)
    return pl.pallas_call(
        final_kernel,
        out_shape=shape_of((rows, width), BF16),
        in_specs=[VMEM] * 4,
        out_specs=VMEM,
        name="final",
        compiler_params=vmem(8),
    )(*held(latent, keep, got, planes))


def solution(mesh):
    torus = Mesh(mesh.devices.reshape(16, 4, 4, 2), ALL)

    return jax.shard_map(
        shards,
        mesh=torus,
        in_specs=(
            P(ALL, None),
            P(SP),
            P(SP),
            P(SP, None),
            P(),
            P(SP, TP),
            P(SP, TP),
            P(SP, TP),
            P(None, TP),
            P(None, TP),
            P(None, TP),
            P(TP),
            P(TP, None),
        ),
        out_specs=P(ALL, None),
        check_vma=False,
    )
```

```python
import jax
import jax.numpy as jnp
from jax import lax
from jax.experimental import pallas as pl
from jax.experimental.pallas import tpu as pltpu
from jax.sharding import Mesh
from jax.sharding import PartitionSpec as P

HEAD_DIM = 128
WINDOW_REACH = 128
GRID_W = 64
SP = ("z", "y")
TP = ("x", "c")
PLANE = ("y", "x", "c")
ALL = ("z", "y", "x", "c")
NORM_EPS = 1e-05
MASKED_SCORE = -1e30
LOG2_E = 1.4426950408889634
CHUNK = 16
SHIFTS = (0, 1, 3, 2)


VMEM = pl.BlockSpec(memory_space=pltpu.VMEM)
SMEM = pl.BlockSpec(memory_space=pltpu.SMEM)
HBM = pl.BlockSpec(memory_space=pltpu.HBM)
F32 = jnp.float32
BF16 = jnp.bfloat16


def shape_of(shape, dtype):
    return jax.ShapeDtypeStruct(shape, dtype)


def vmem(mib):
    return pltpu.CompilerParams(vmem_limit_bytes=mib * 2**20)


def held(*arrays):
    return [pltpu.with_memory_space_constraint(a, pltpu.VMEM) for a in arrays]


def far(*arrays):
    return [pltpu.with_memory_space_constraint(a, pltpu.HBM) for a in arrays]


def exchanged(blocks, axis):
    return lax.all_to_all(blocks, axis, 0, 0, tiled=True)


def dot(a, b):
    return jnp.dot(a, b, preferred_element_type=F32)


def row_vector(planes_ref, index, columns):
    count = planes_ref.shape[0] // 4
    cut = pl.ds(index * columns, columns)
    pieces = []
    for t in range(count):
        piece = planes_ref[t, :, cut]
        for y in range(1, 4):
            piece = piece + planes_ref[y * count + t, :, cut]
        pieces.append(piece)
    return jnp.concatenate(pieces, axis=1)


def parts_kernel(
    cond_ref, ctx_cond_ref, shift_ref, scale_ref, gate_ref, ctx_ref, gain_ref,
    out_ref, ctx_held_ref, gain_held_ref,
):
    def active(ref):
        v = ref[...]
        return (v / (1.0 + jnp.exp(-v))).astype(BF16)

    both = jnp.concatenate([active(cond_ref), active(ctx_cond_ref)], axis=0)
    both = jnp.concatenate([both, jnp.zeros((14, both.shape[1]), BF16)], axis=0)
    shift = dot(both, shift_ref[...])
    scale = dot(both, scale_ref[...])
    gate = dot(both, gate_ref[...])
    row = jnp.concatenate([shift[0:1], shift[1:2], scale[0:1], scale[1:2], gate[0:1]], axis=1)
    for i in range(out_ref.shape[0]):
        out_ref[i] = row
    ctx_held_ref[...] = ctx_ref[...]
    gain_held_ref[...] = gain_ref[...]


def normed_rows(ref, x, start, multiplier, shift):
    rows = ref[x, pl.ds(start, CHUNK), :].astype(F32)
    mean = jnp.mean(rows * rows, axis=-1, keepdims=True)
    return (rows * lax.rsqrt(mean + NORM_EPS) * multiplier + shift).astype(BF16)


def turned(u, cosine, sine):
    lane = lax.broadcasted_iota(jnp.int32, u.shape, 1)
    first = (lane % 64) < 32
    swapped = jnp.where(first, pltpu.roll(u, 96, 1), pltpu.roll(u, 32, 1))
    return u * cosine + swapped * sine


def sum_kernel(parts_ref, out_ref):
    total = parts_ref[0]
    for z in range(1, parts_ref.shape[0]):
        total = total + parts_ref[z]
    for p in range(out_ref.shape[0]):
        out_ref[p] = total


def qkv_kernel(
    place_ref, own_ref, other_ref, planes_ref, gain_ref, wq_ref, wk_ref, wv_ref, row_ref, col_ref,
    q_ref, kv_ref, top_ref, bottom_ref, hidden_ref, wq_held_ref, wkv_ref, halves_ref, sems,
):
    columns = wq_ref.shape[1]
    loads = (
        pltpu.make_async_copy(wq_ref, wq_held_ref, sems.at[0]),
        pltpu.make_async_copy(wk_ref, halves_ref.at[0], sems.at[1]),
        pltpu.make_async_copy(wv_ref, halves_ref.at[1], sems.at[2]),
    )
    for load in loads:
        load.start()
    shift = row_vector(planes_ref, 0, columns)
    multiplier = gain_ref[...] * (1.0 + row_vector(planes_ref, 2, columns))
    _, rows, _ = own_ref.shape
    at_x, core = place_ref[0], place_ref[1]
    for x, shift_x in enumerate(SHIFTS):
        source = lax.rem(at_x - shift_x + 4, 4)
        mine = (2 * source + core) * rows
        theirs = (2 * source + 1 - core) * rows

        def step(i, carry, x=x, mine=mine, theirs=theirs):
            start = pl.multiple_of(i * CHUNK, CHUNK)
            at = pl.multiple_of(mine + start, CHUNK)
            hidden_ref[pl.ds(at, CHUNK), :] = normed_rows(own_ref, x, start, multiplier, shift)
            at = pl.multiple_of(theirs + start, CHUNK)
            hidden_ref[pl.ds(at, CHUNK), :] = normed_rows(other_ref, x, start, multiplier, shift)
            return carry

        lax.fori_loop(0, rows // CHUNK, step, 0, unroll=2)
    for load in loads:
        load.wait()
    wkv_ref[:, :HEAD_DIM] = halves_ref[0]
    wkv_ref[:, HEAD_DIM:] = halves_ref[1]
    block = 384
    lane = lax.broadcasted_iota(jnp.int32, (GRID_W, HEAD_DIM), 1) < 64
    col = col_ref[...]
    col_turned = pltpu.roll(col, 64, 1)
    row_turned = pltpu.roll(row_ref[...], 64, 1)
    factor = HEAD_DIM ** (-0.5) * LOG2_E
    for at in range(0, hidden_ref.shape[0], block):
        cut = slice(at, at + block)
        hidden = hidden_ref[cut, :]
        lines = range(at // GRID_W, (at + block) // GRID_W)
        cosine = jnp.concatenate(
            [jnp.where(lane, row_ref[g : g + 1, :], col_turned) for g in lines], axis=0
        )
        sine = jnp.concatenate(
            [jnp.where(lane, row_turned[g : g + 1, :], col) for g in lines], axis=0
        )
        queries = dot(hidden, wq_held_ref[...])
        for h in range(2):
            part = slice(h * HEAD_DIM, (h + 1) * HEAD_DIM)
            q_ref[cut, part] = (turned(queries[:, part], cosine, sine) * factor).astype(BF16)
        pairs = dot(hidden, wkv_ref[...])
        kv_ref[cut, :HEAD_DIM] = turned(pairs[:, :HEAD_DIM], cosine, sine).astype(BF16)
        kv_ref[cut, HEAD_DIM:] = pairs[:, HEAD_DIM:].astype(BF16)
    top_ref[...] = kv_ref[:WINDOW_REACH, :]
    bottom_ref[...] = kv_ref[hidden_ref.shape[0] - WINDOW_REACH :, :]


def context_kernel(ctx_ref, planes_ref, gain_ref, wk_ref, wv_ref, out_ref):
    columns = planes_ref.shape[2] // 5
    shift = row_vector(planes_ref, 1, columns)
    multiplier = gain_ref[...] * (1.0 + row_vector(planes_ref, 3, columns))
    rows = ctx_ref[...].astype(F32)
    mean = jnp.mean(rows * rows, axis=-1, keepdims=True)
    hidden = (rows * lax.rsqrt(mean + NORM_EPS) * multiplier + shift).astype(BF16)
    pairs = jnp.concatenate([dot(hidden, wk_ref[...]), dot(hidden, wv_ref[...])], axis=1)
    pairs = pairs.astype(BF16)
    for p in range(out_ref.shape[0]):
        out_ref[p] = pairs


def spread_kernel(block_ref, out_ref, sems):
    sends = [
        pltpu.make_async_copy(block_ref, out_ref.at[y], sems.at[y])
        for y in range(out_ref.shape[0])
    ]
    for send in sends:
        send.start()
    for send in sends:
        send.wait()


def attention_kernel(
    place_ref, sink_ref, q_ref, low_ref, kv_ref, high_ref, ctx_ref, attended_ref,
    keys_ref, values_ref, ctx_values_ref,
):
    reach = WINDOW_REACH
    total = kv_ref.shape[0]
    first, last = place_ref[2], place_ref[3]
    for ref, at in ((low_ref, 0), (kv_ref, reach), (high_ref, reach + total)):
        cut = slice(at, at + ref.shape[0])
        keys_ref[cut, :] = ref[:, :HEAD_DIM]
        values_ref[cut, :HEAD_DIM] = ref[:, HEAD_DIM:]
    values_ref[:, HEAD_DIM:] = jnp.ones(keys_ref.shape, BF16)
    ctx_values_ref[:, :HEAD_DIM] = ctx_ref[:, HEAD_DIM:]
    ctx_values_ref[:, HEAD_DIM:] = jnp.ones((ctx_ref.shape[0], HEAD_DIM), BF16)
    row = lax.broadcasted_iota(jnp.int32, (2 * reach, 1), 0)
    sink = jnp.where(row < reach, sink_ref[0], sink_ref[1]) * LOG2_E
    position = lax.broadcasted_iota(jnp.int32, (2 * reach, 3 * reach), 0) % reach
    column = lax.broadcasted_iota(jnp.int32, (2 * reach, 3 * reach), 1)
    band = (column >= position) & (column <= position + 2 * reach)
    blocks = total // reach
    contract = (((1,), (1,)), ((), ()))

    def step(b, carry):
        at = pl.multiple_of(b * reach, reach)
        both = q_ref[pl.ds(at, reach), :]
        queries = jnp.concatenate([both[:, :HEAD_DIM], both[:, HEAD_DIM:]], axis=0)
        keys = keys_ref[pl.ds(at, 3 * reach), :]
        values = values_ref[pl.ds(at, 3 * reach), :]
        lowest = jnp.where(b == 0, first * reach, 0)
        highest = jnp.where(b == blocks - 1, (3 - last) * reach, 3 * reach)
        allowed = band & (column >= lowest) & (column < highest)
        near = lax.dot_general(queries, keys, contract, preferred_element_type=F32)
        near = jnp.where(allowed, near, MASKED_SCORE)
        far = lax.dot_general(
            queries, ctx_ref[:, :HEAD_DIM], contract, preferred_element_type=F32
        )
        top = jnp.maximum(
            jnp.max(near, axis=-1, keepdims=True), jnp.max(far, axis=-1, keepdims=True)
        )
        top = jnp.maximum(top, sink)
        near = jnp.exp2(near - top).astype(BF16)
        far = jnp.exp2(far - top).astype(BF16)
        mixed = dot(near, values) + dot(far, ctx_values_ref[...])
        share = mixed[:, HEAD_DIM:] + jnp.exp2(sink - top)
        mixed = (mixed[:, :HEAD_DIM] / share).astype(BF16)
        attended_ref[pl.ds(at, reach), :HEAD_DIM] = mixed[:reach]
        attended_ref[pl.ds(at, reach), HEAD_DIM:] = mixed[reach:]
        return carry

    lax.fori_loop(0, blocks, step, 0, unroll=True)


def load_kernel(w0_ref, w1_ref, out_ref, sems):
    loads = [
        pltpu.make_async_copy(w, out_ref.at[j], sems.at[j])
        for j, w in enumerate((w0_ref, w1_ref))
    ]
    for load in loads:
        load.start()
    for load in loads:
        load.wait()


def project_kernel(
    place_ref, attended_ref, early_ref, w2_ref, w3_ref, send_ref, keep_ref,
    rows_ref, late_ref, sems,
):
    width = 512
    cuts = [slice(n, n + width) for n in range(0, send_ref.shape[1], width)]
    loads = [
        [
            pltpu.make_async_copy(w.at[:, cut], late_ref.at[j, :, cut], sems.at[n, j])
            for j, w in enumerate((w2_ref, w3_ref))
        ]
        for n, cut in enumerate(cuts)
    ]
    for group in loads:
        for load in group:
            load.start()
    at_x, core = place_ref[0], place_ref[1]
    rows = send_ref.shape[0]
    deep = attended_ref.shape[2]
    mine = pl.multiple_of(core * rows, CHUNK)
    theirs = pl.multiple_of((1 - core) * rows, CHUNK)
    for j, shift_x in enumerate(SHIFTS):
        source = lax.rem(at_x - shift_x + 4, 4)
        cut = slice(j * deep, (j + 1) * deep)
        rows_ref[:rows, cut] = attended_ref[source, pl.ds(theirs, rows), :]
        rows_ref[rows:, cut] = attended_ref[source, pl.ds(mine, rows), :]
    for group, cut in zip(loads, cuts):
        total = dot(rows_ref[:, :deep], early_ref[0, :, cut])
        total = total + dot(rows_ref[:, deep : 2 * deep], early_ref[1, :, cut])
        for load in group:
            load.wait()
        for j in range(2):
            part = slice((2 + j) * deep, (3 + j) * deep)
            total = total + dot(rows_ref[:, part], late_ref[j, :, cut])
        send_ref[:, cut] = total[:rows].astype(BF16)
        keep_ref[:, cut] = total[rows:]


def final_kernel(latent_ref, keep_ref, got_ref, planes_ref, out_ref):
    gate = row_vector(planes_ref, 4, planes_ref.shape[2] // 5)

    def step(i, carry):
        cut = pl.ds(pl.multiple_of(i * CHUNK, CHUNK), CHUNK)
        mixed = keep_ref[cut, :] + got_ref[cut, :].astype(F32)
        out_ref[cut, :] = (latent_ref[cut, :].astype(F32) + gate * mixed).astype(BF16)
        return carry

    lax.fori_loop(0, latent_ref.shape[0] // CHUNK, step, 0)


def from_other_x(block):
    got = []
    for shift in SHIFTS[1:]:
        got.append(lax.ppermute(block, "x", [(i, (i + shift) % 4) for i in range(4)]))
    return got


def swapped(x):
    return lax.ppermute(x, "c", [(0, 1), (1, 0)])


def tables(first_line, lines):
    inv_freq = 10000.0 ** (-jnp.arange(0, HEAD_DIM // 2, 2, dtype=F32) / (HEAD_DIM // 2))
    at = jnp.concatenate([first_line + jnp.arange(lines), jnp.arange(GRID_W)])
    angles = at.astype(F32)[:, None] * inv_freq
    cosine, sine = jnp.cos(angles), jnp.sin(angles)
    table = jnp.concatenate([cosine, cosine, -sine, sine], axis=1)
    return table[:lines], table[lines:]


def shards(
    latent,
    condition,
    context_condition,
    context,
    norm_gain,
    shift_weight,
    scale_weight,
    gate_weight,
    query_weight,
    key_matrix,
    value_matrix,
    sink_logit_head,
    out_weight,
):
    nz, ny, nx, nc = (lax.axis_size(a) for a in ALL)
    rows, width = latent.shape
    group_rows = rows * nx * nc
    columns = shift_weight.shape[1]
    place = lax.axis_index(SP)
    gain = norm_gain.reshape(1, width)
    parts, context, gain = pl.pallas_call(
        parts_kernel,
        out_shape=[
            shape_of((nz, 1, 5 * columns), F32),
            pltpu.VMEM(context.shape, BF16),
            pltpu.VMEM((1, width), F32),
        ],
        in_specs=[VMEM] * 7,
        out_specs=[VMEM] * 3,
        name="parts",
        compiler_params=vmem(6),
    )(
        *far(condition.reshape(1, -1), context_condition.reshape(1, -1)),
        *far(shift_weight, scale_weight, gate_weight, context, gain),
    )
    parts = exchanged(parts, "z")
    latent_others = from_other_x(latent)
    lines, cols = tables(place * (group_rows // GRID_W), group_rows // GRID_W)
    count = nz * ny
    where = jnp.stack(
        [
            lax.axis_index("x").astype(jnp.int32),
            lax.axis_index("c").astype(jnp.int32),
            (place == 0).astype(jnp.int32),
            (place == count - 1).astype(jnp.int32),
        ]
    )
    members = ny * nx * nc
    sums = pl.pallas_call(
        sum_kernel,
        out_shape=shape_of((members, 1, 5 * columns), F32),
        in_specs=[VMEM],
        out_specs=VMEM,
        name="sums",
        compiler_params=vmem(4),
    )(*held(parts))
    planes = exchanged(sums, PLANE)
    out_others = from_other_x(out_weight)
    latent_x = jnp.stack([latent, *latent_others])
    latent_c = swapped(latent_x)
    ctx_rows = context.shape[0]
    pairs = pl.pallas_call(
        context_kernel,
        out_shape=shape_of((nz, ctx_rows, 2 * HEAD_DIM), BF16),
        in_specs=[VMEM] * 5,
        out_specs=VMEM,
        name="context_pairs",
        compiler_params=vmem(8),
    )(*held(context, planes, gain, key_matrix, value_matrix))
    ctx_z = exchanged(pairs, "z").reshape(nz * ctx_rows, 2 * HEAD_DIM)
    spread = pl.pallas_call(
        spread_kernel,
        out_shape=pltpu.HBM((ny, *ctx_z.shape), BF16),
        in_specs=[VMEM],
        out_specs=HBM,
        scratch_shapes=[pltpu.SemaphoreType.DMA((ny,))],
        name="spread",
        compiler_params=vmem(4),
    )(*held(ctx_z))
    ctx_pairs = exchanged(spread, "y").reshape(-1, 2 * HEAD_DIM)
    wide = (group_rows, 2 * HEAD_DIM)
    edge = (WINDOW_REACH, 2 * HEAD_DIM)
    queries, pairs, top, bottom = pl.pallas_call(
        qkv_kernel,
        out_shape=[pltpu.VMEM(shape, BF16) for shape in (wide, wide, edge, edge)],
        in_specs=[SMEM] + [VMEM] * 4 + [HBM] * 3 + [VMEM] * 2,
        out_specs=[VMEM] * 4,
        scratch_shapes=[
            pltpu.VMEM((group_rows, width), BF16),
            pltpu.VMEM((width, 2 * HEAD_DIM), BF16),
            pltpu.VMEM((width, 2 * HEAD_DIM), BF16),
            pltpu.VMEM((2, width, HEAD_DIM), BF16),
            pltpu.SemaphoreType.DMA((3,)),
        ],
        name="qkv",
        compiler_params=vmem(20),
    )(
        where,
        *held(latent_x, latent_c, planes, gain),
        *far(query_weight, key_matrix, value_matrix),
        *held(lines, cols),
    )
    low = lax.ppermute(bottom, SP, [(i, i + 1) for i in range(count - 1)])
    high = lax.ppermute(top, SP, [(i + 1, i) for i in range(count - 1)])
    long = group_rows + 2 * WINDOW_REACH
    attended = pl.pallas_call(
        attention_kernel,
        out_shape=shape_of(wide, BF16),
        in_specs=[SMEM] * 2 + [VMEM] * 5,
        out_specs=VMEM,
        scratch_shapes=[
            pltpu.VMEM((long, HEAD_DIM), BF16),
            pltpu.VMEM((long, 2 * HEAD_DIM), BF16),
            pltpu.VMEM((count * ctx_rows, 2 * HEAD_DIM), BF16),
        ],
        name="attention",
        compiler_params=vmem(16),
    )(where, sink_logit_head, *held(queries, low, pairs, high, ctx_pairs))
    attended = exchanged(attended.reshape(nx, nc * rows, 2 * HEAD_DIM), "x")
    weights = pl.pallas_call(
        load_kernel,
        out_shape=pltpu.VMEM((2, *out_weight.shape), BF16),
        in_specs=[HBM] * 2,
        out_specs=VMEM,
        scratch_shapes=[pltpu.SemaphoreType.DMA((2,))],
        name="load",
        compiler_params=vmem(2),
    )(*far(out_weight, out_others[0]))
    send, keep = pl.pallas_call(
        project_kernel,
        out_shape=[pltpu.VMEM((rows, width), BF16), pltpu.VMEM((rows, width), F32)],
        in_specs=[SMEM, VMEM, VMEM, HBM, HBM],
        out_specs=(VMEM, VMEM),
        scratch_shapes=[
            pltpu.VMEM((nc * rows, nx * 2 * HEAD_DIM), BF16),
            pltpu.VMEM((2, 2 * HEAD_DIM, width), BF16),
            pltpu.SemaphoreType.DMA((4, 2)),
        ],
        name="project",
        compiler_params=vmem(14),
    )(where, *held(attended, weights), *far(*out_others[1:]))
    got = swapped(send)
    return pl.pallas_call(
        final_kernel,
        out_shape=shape_of((rows, width), BF16),
        in_specs=[VMEM] * 4,
        out_specs=VMEM,
        name="final",
        compiler_params=vmem(8),
    )(*held(latent, keep, got, planes))


def solution(mesh):
    torus = Mesh(mesh.devices.reshape(16, 4, 4, 2), ALL)

    return jax.shard_map(
        shards,
        mesh=torus,
        in_specs=(
            P(ALL, None),
            P(SP),
            P(SP),
            P(SP, None),
            P(),
            P(SP, TP),
            P(SP, TP),
            P(SP, TP),
            P(None, TP),
            P(None, TP),
            P(None, TP),
            P(TP),
            P(TP, None),
        ),
        out_specs=P(ALL, None),
        check_vma=False,
    )
```

```python
import jax
import jax.numpy as jnp
from jax import lax
from jax.experimental import pallas as pl
from jax.experimental.pallas import tpu as pltpu
from jax.sharding import Mesh
from jax.sharding import PartitionSpec as P

HEAD_DIM = 128
WINDOW_REACH = 128
GRID_W = 64
SP = ("z", "y")
TP = ("x", "c")
PLANE = ("y", "x", "c")
ALL = ("z", "y", "x", "c")
NORM_EPS = 1e-05
MASKED_SCORE = -1e30
LOG2_E = 1.4426950408889634
CHUNK = 16
SHIFTS = (0, 1, 3, 2)


VMEM = pl.BlockSpec(memory_space=pltpu.VMEM)
SMEM = pl.BlockSpec(memory_space=pltpu.SMEM)
HBM = pl.BlockSpec(memory_space=pltpu.HBM)
F32 = jnp.float32
BF16 = jnp.bfloat16


def shape_of(shape, dtype):
    return jax.ShapeDtypeStruct(shape, dtype)


def vmem(mib):
    return pltpu.CompilerParams(vmem_limit_bytes=mib * 2**20)


def held(*arrays):
    return [pltpu.with_memory_space_constraint(a, pltpu.VMEM) for a in arrays]


def far(*arrays):
    return [pltpu.with_memory_space_constraint(a, pltpu.HBM) for a in arrays]


def exchanged(blocks, axis):
    return lax.all_to_all(blocks, axis, 0, 0, tiled=True)


def dot(a, b):
    return jnp.dot(a, b, preferred_element_type=F32)


def row_vector(planes_ref, index, columns):
    count = planes_ref.shape[0] // 4
    cut = pl.ds(index * columns, columns)
    pieces = []
    for t in range(count):
        piece = planes_ref[t, :, cut]
        for y in range(1, 4):
            piece = piece + planes_ref[y * count + t, :, cut]
        pieces.append(piece)
    return jnp.concatenate(pieces, axis=1)


def parts_kernel(
    cond_ref, ctx_cond_ref, shift_ref, scale_ref, gate_ref, ctx_ref, gain_ref,
    out_ref, ctx_held_ref, gain_held_ref,
):
    def active(ref):
        v = ref[...]
        return (v / (1.0 + jnp.exp(-v))).astype(BF16)

    both = jnp.concatenate([active(cond_ref), active(ctx_cond_ref)], axis=0)
    both = jnp.concatenate([both, jnp.zeros((14, both.shape[1]), BF16)], axis=0)
    shift = dot(both, shift_ref[...])
    scale = dot(both, scale_ref[...])
    gate = dot(both, gate_ref[...])
    row = jnp.concatenate([shift[0:1], shift[1:2], scale[0:1], scale[1:2], gate[0:1]], axis=1)
    half = out_ref.shape[2]
    row = jnp.concatenate([row[:, :half], row[:, half:]], axis=0).astype(BF16)
    for i in range(out_ref.shape[0]):
        out_ref[i] = row
    ctx_held_ref[...] = ctx_ref[...]
    gain_held_ref[...] = gain_ref[...]


def normed_rows(ref, x, start, multiplier, shift):
    rows = ref[x, pl.ds(start, CHUNK), :].astype(F32)
    mean = jnp.mean(rows * rows, axis=-1, keepdims=True)
    return (rows * lax.rsqrt(mean + NORM_EPS) * multiplier + shift).astype(BF16)


def turned(u, cosine, sine):
    lane = lax.broadcasted_iota(jnp.int32, u.shape, 1)
    first = (lane % 64) < 32
    swapped = jnp.where(first, pltpu.roll(u, 96, 1), pltpu.roll(u, 32, 1))
    return u * cosine + swapped * sine


def sum_kernel(parts_ref, out_ref):
    total = parts_ref[0].astype(F32)
    for z in range(1, parts_ref.shape[0]):
        total = total + parts_ref[z].astype(F32)
    total = jnp.concatenate([total[0:1], total[1:2]], axis=1)
    for p in range(out_ref.shape[0]):
        out_ref[p] = total


def qkv_kernel(
    place_ref, own_ref, other_ref, planes_ref, gain_ref, wq_ref, wk_ref, wv_ref, row_ref, col_ref,
    q_ref, kv_ref, top_ref, bottom_ref, hidden_ref, wq_held_ref, wkv_ref, halves_ref, sems,
):
    columns = wq_ref.shape[1]
    loads = (
        pltpu.make_async_copy(wq_ref, wq_held_ref, sems.at[0]),
        pltpu.make_async_copy(wk_ref, halves_ref.at[0], sems.at[1]),
        pltpu.make_async_copy(wv_ref, halves_ref.at[1], sems.at[2]),
    )
    for load in loads:
        load.start()
    shift = row_vector(planes_ref, 0, columns)
    multiplier = gain_ref[...] * (1.0 + row_vector(planes_ref, 2, columns))
    _, rows, _ = own_ref.shape
    at_x, core = place_ref[0], place_ref[1]
    for x, shift_x in enumerate(SHIFTS):
        source = lax.rem(at_x - shift_x + 4, 4)
        mine = (2 * source + core) * rows
        theirs = (2 * source + 1 - core) * rows

        def step(i, carry, x=x, mine=mine, theirs=theirs):
            start = pl.multiple_of(i * CHUNK, CHUNK)
            at = pl.multiple_of(mine + start, CHUNK)
            hidden_ref[pl.ds(at, CHUNK), :] = normed_rows(own_ref, x, start, multiplier, shift)
            at = pl.multiple_of(theirs + start, CHUNK)
            hidden_ref[pl.ds(at, CHUNK), :] = normed_rows(other_ref, x, start, multiplier, shift)
            return carry

        lax.fori_loop(0, rows // CHUNK, step, 0, unroll=2)
    for load in loads:
        load.wait()
    wkv_ref[:, :HEAD_DIM] = halves_ref[0]
    wkv_ref[:, HEAD_DIM:] = halves_ref[1]
    block = 384
    lane = lax.broadcasted_iota(jnp.int32, (GRID_W, HEAD_DIM), 1) < 64
    col = col_ref[...]
    col_turned = pltpu.roll(col, 64, 1)
    row_turned = pltpu.roll(row_ref[...], 64, 1)
    factor = HEAD_DIM ** (-0.5) * LOG2_E
    for at in range(0, hidden_ref.shape[0], block):
        cut = slice(at, at + block)
        hidden = hidden_ref[cut, :]
        lines = range(at // GRID_W, (at + block) // GRID_W)
        cosine = jnp.concatenate(
            [jnp.where(lane, row_ref[g : g + 1, :], col_turned) for g in lines], axis=0
        )
        sine = jnp.concatenate(
            [jnp.where(lane, row_turned[g : g + 1, :], col) for g in lines], axis=0
        )
        queries = dot(hidden, wq_held_ref[...])
        for h in range(2):
            part = slice(h * HEAD_DIM, (h + 1) * HEAD_DIM)
            q_ref[cut, part] = (turned(queries[:, part], cosine, sine) * factor).astype(BF16)
        pairs = dot(hidden, wkv_ref[...])
        kv_ref[cut, :HEAD_DIM] = turned(pairs[:, :HEAD_DIM], cosine, sine).astype(BF16)
        kv_ref[cut, HEAD_DIM:] = pairs[:, HEAD_DIM:].astype(BF16)
    top_ref[...] = kv_ref[:WINDOW_REACH, :]
    bottom_ref[...] = kv_ref[hidden_ref.shape[0] - WINDOW_REACH :, :]


def context_kernel(ctx_ref, planes_ref, gain_ref, wk_ref, wv_ref, out_ref):
    columns = planes_ref.shape[2] // 5
    shift = row_vector(planes_ref, 1, columns)
    multiplier = gain_ref[...] * (1.0 + row_vector(planes_ref, 3, columns))
    rows = ctx_ref[...].astype(F32)
    mean = jnp.mean(rows * rows, axis=-1, keepdims=True)
    hidden = (rows * lax.rsqrt(mean + NORM_EPS) * multiplier + shift).astype(BF16)
    pairs = jnp.concatenate([dot(hidden, wk_ref[...]), dot(hidden, wv_ref[...])], axis=1)
    pairs = pairs.astype(BF16)
    for p in range(out_ref.shape[0]):
        out_ref[p] = pairs


def spread_kernel(block_ref, out_ref, sems):
    sends = [
        pltpu.make_async_copy(block_ref, out_ref.at[y], sems.at[y])
        for y in range(out_ref.shape[0])
    ]
    for send in sends:
        send.start()
    for send in sends:
        send.wait()


def attention_kernel(
    place_ref, sink_ref, q_ref, low_ref, kv_ref, high_ref, ctx_ref, attended_ref,
    keys_ref, values_ref, ctx_values_ref,
):
    reach = WINDOW_REACH
    total = kv_ref.shape[0]
    first, last = place_ref[2], place_ref[3]
    for ref, at in ((low_ref, 0), (kv_ref, reach), (high_ref, reach + total)):
        cut = slice(at, at + ref.shape[0])
        keys_ref[cut, :] = ref[:, :HEAD_DIM]
        values_ref[cut, :HEAD_DIM] = ref[:, HEAD_DIM:]
    values_ref[:, HEAD_DIM:] = jnp.ones(keys_ref.shape, BF16)
    ctx_values_ref[:, :HEAD_DIM] = ctx_ref[:, HEAD_DIM:]
    ctx_values_ref[:, HEAD_DIM:] = jnp.ones((ctx_ref.shape[0], HEAD_DIM), BF16)
    row = lax.broadcasted_iota(jnp.int32, (2 * reach, 1), 0)
    sink = jnp.where(row < reach, sink_ref[0], sink_ref[1]) * LOG2_E
    position = lax.broadcasted_iota(jnp.int32, (2 * reach, 3 * reach), 0) % reach
    column = lax.broadcasted_iota(jnp.int32, (2 * reach, 3 * reach), 1)
    band = (column >= position) & (column <= position + 2 * reach)
    blocks = total // reach
    contract = (((1,), (1,)), ((), ()))

    def step(b, carry):
        at = pl.multiple_of(b * reach, reach)
        both = q_ref[pl.ds(at, reach), :]
        queries = jnp.concatenate([both[:, :HEAD_DIM], both[:, HEAD_DIM:]], axis=0)
        keys = keys_ref[pl.ds(at, 3 * reach), :]
        values = values_ref[pl.ds(at, 3 * reach), :]
        lowest = jnp.where(b == 0, first * reach, 0)
        highest = jnp.where(b == blocks - 1, (3 - last) * reach, 3 * reach)
        allowed = band & (column >= lowest) & (column < highest)
        near = lax.dot_general(queries, keys, contract, preferred_element_type=F32)
        near = jnp.where(allowed, near, MASKED_SCORE)
        far = lax.dot_general(
            queries, ctx_ref[:, :HEAD_DIM], contract, preferred_element_type=F32
        )
        top = jnp.maximum(
            jnp.max(near, axis=-1, keepdims=True), jnp.max(far, axis=-1, keepdims=True)
        )
        top = jnp.maximum(top, sink)
        near = jnp.exp2(near - top).astype(BF16)
        far = jnp.exp2(far - top).astype(BF16)
        mixed = dot(near, values) + dot(far, ctx_values_ref[...])
        share = mixed[:, HEAD_DIM:] + jnp.exp2(sink - top)
        mixed = (mixed[:, :HEAD_DIM] / share).astype(BF16)
        attended_ref[pl.ds(at, reach), :HEAD_DIM] = mixed[:reach]
        attended_ref[pl.ds(at, reach), HEAD_DIM:] = mixed[reach:]
        return carry

    lax.fori_loop(0, blocks, step, 0, unroll=True)


def load_kernel(w0_ref, w1_ref, out_ref, sems):
    loads = [
        pltpu.make_async_copy(w, out_ref.at[j], sems.at[j])
        for j, w in enumerate((w0_ref, w1_ref))
    ]
    for load in loads:
        load.start()
    for load in loads:
        load.wait()


def project_kernel(
    place_ref, attended_ref, early_ref, w2_ref, w3_ref, send_ref, keep_ref,
    rows_ref, late_ref, sems,
):
    width = 512
    cuts = [slice(n, n + width) for n in range(0, send_ref.shape[1], width)]
    loads = [
        [
            pltpu.make_async_copy(w.at[:, cut], late_ref.at[j, :, cut], sems.at[n, j])
            for j, w in enumerate((w2_ref, w3_ref))
        ]
        for n, cut in enumerate(cuts)
    ]
    for group in loads:
        for load in group:
            load.start()
    at_x, core = place_ref[0], place_ref[1]
    rows = send_ref.shape[0]
    deep = attended_ref.shape[2]
    mine = pl.multiple_of(core * rows, CHUNK)
    theirs = pl.multiple_of((1 - core) * rows, CHUNK)
    for j, shift_x in enumerate(SHIFTS):
        source = lax.rem(at_x - shift_x + 4, 4)
        cut = slice(j * deep, (j + 1) * deep)
        rows_ref[:rows, cut] = attended_ref[source, pl.ds(theirs, rows), :]
        rows_ref[rows:, cut] = attended_ref[source, pl.ds(mine, rows), :]
    for group, cut in zip(loads, cuts):
        total = dot(rows_ref[:, :deep], early_ref[0, :, cut])
        total = total + dot(rows_ref[:, deep : 2 * deep], early_ref[1, :, cut])
        for load in group:
            load.wait()
        for j in range(2):
            part = slice((2 + j) * deep, (3 + j) * deep)
            total = total + dot(rows_ref[:, part], late_ref[j, :, cut])
        send_ref[:, cut] = total[:rows].astype(BF16)
        keep_ref[:, cut] = total[rows:]


def final_kernel(latent_ref, keep_ref, got_ref, planes_ref, out_ref):
    gate = row_vector(planes_ref, 4, planes_ref.shape[2] // 5)

    def step(i, carry):
        cut = pl.ds(pl.multiple_of(i * CHUNK, CHUNK), CHUNK)
        mixed = keep_ref[cut, :] + got_ref[cut, :].astype(F32)
        out_ref[cut, :] = (latent_ref[cut, :].astype(F32) + gate * mixed).astype(BF16)
        return carry

    lax.fori_loop(0, latent_ref.shape[0] // CHUNK, step, 0)


def from_other_x(block):
    got = []
    for shift in SHIFTS[1:]:
        got.append(lax.ppermute(block, "x", [(i, (i + shift) % 4) for i in range(4)]))
    return got


def swapped(x):
    return lax.ppermute(x, "c", [(0, 1), (1, 0)])


def tables(first_line, lines):
    inv_freq = 10000.0 ** (-jnp.arange(0, HEAD_DIM // 2, 2, dtype=F32) / (HEAD_DIM // 2))
    at = jnp.concatenate([first_line + jnp.arange(lines), jnp.arange(GRID_W)])
    angles = at.astype(F32)[:, None] * inv_freq
    cosine, sine = jnp.cos(angles), jnp.sin(angles)
    table = jnp.concatenate([cosine, cosine, -sine, sine], axis=1)
    return table[:lines], table[lines:]


def shards(
    latent,
    condition,
    context_condition,
    context,
    norm_gain,
    shift_weight,
    scale_weight,
    gate_weight,
    query_weight,
    key_matrix,
    value_matrix,
    sink_logit_head,
    out_weight,
):
    nz, ny, nx, nc = (lax.axis_size(a) for a in ALL)
    rows, width = latent.shape
    group_rows = rows * nx * nc
    columns = shift_weight.shape[1]
    place = lax.axis_index(SP)
    gain = norm_gain.reshape(1, width)
    parts, context, gain = pl.pallas_call(
        parts_kernel,
        out_shape=[
            shape_of((nz, 2, 5 * columns // 2), BF16),
            pltpu.VMEM(context.shape, BF16),
            pltpu.VMEM((1, width), F32),
        ],
        in_specs=[VMEM] * 7,
        out_specs=[VMEM] * 3,
        name="parts",
        compiler_params=vmem(6),
    )(
        *far(condition.reshape(1, -1), context_condition.reshape(1, -1)),
        *far(shift_weight, scale_weight, gate_weight, context, gain),
    )
    parts = exchanged(parts, "z")
    latent_others = from_other_x(latent)
    lines, cols = tables(place * (group_rows // GRID_W), group_rows // GRID_W)
    count = nz * ny
    where = jnp.stack(
        [
            lax.axis_index("x").astype(jnp.int32),
            lax.axis_index("c").astype(jnp.int32),
            (place == 0).astype(jnp.int32),
            (place == count - 1).astype(jnp.int32),
        ]
    )
    members = ny * nx * nc
    sums = pl.pallas_call(
        sum_kernel,
        out_shape=shape_of((members, 1, 5 * columns), F32),
        in_specs=[VMEM],
        out_specs=VMEM,
        name="sums",
        compiler_params=vmem(4),
    )(*held(parts))
    planes = exchanged(sums, PLANE)
    out_others = from_other_x(out_weight)
    latent_x = jnp.stack([latent, *latent_others])
    latent_c = swapped(latent_x)
    ctx_rows = context.shape[0]
    pairs = pl.pallas_call(
        context_kernel,
        out_shape=shape_of((nz, ctx_rows, 2 * HEAD_DIM), BF16),
        in_specs=[VMEM] * 5,
        out_specs=VMEM,
        name="context_pairs",
        compiler_params=vmem(8),
    )(*held(context, planes, gain, key_matrix, value_matrix))
    ctx_z = exchanged(pairs, "z").reshape(nz * ctx_rows, 2 * HEAD_DIM)
    spread = pl.pallas_call(
        spread_kernel,
        out_shape=pltpu.HBM((ny, *ctx_z.shape), BF16),
        in_specs=[VMEM],
        out_specs=HBM,
        scratch_shapes=[pltpu.SemaphoreType.DMA((ny,))],
        name="spread",
        compiler_params=vmem(4),
    )(*held(ctx_z))
    ctx_pairs = exchanged(spread, "y").reshape(-1, 2 * HEAD_DIM)
    wide = (group_rows, 2 * HEAD_DIM)
    edge = (WINDOW_REACH, 2 * HEAD_DIM)
    queries, pairs, top, bottom = pl.pallas_call(
        qkv_kernel,
        out_shape=[pltpu.VMEM(shape, BF16) for shape in (wide, wide, edge, edge)],
        in_specs=[SMEM] + [VMEM] * 4 + [HBM] * 3 + [VMEM] * 2,
        out_specs=[VMEM] * 4,
        scratch_shapes=[
            pltpu.VMEM((group_rows, width), BF16),
            pltpu.VMEM((width, 2 * HEAD_DIM), BF16),
            pltpu.VMEM((width, 2 * HEAD_DIM), BF16),
            pltpu.VMEM((2, width, HEAD_DIM), BF16),
            pltpu.SemaphoreType.DMA((3,)),
        ],
        name="qkv",
        compiler_params=vmem(20),
    )(
        where,
        *held(latent_x, latent_c, planes, gain),
        *far(query_weight, key_matrix, value_matrix),
        *held(lines, cols),
    )
    low = lax.ppermute(bottom, SP, [(i, i + 1) for i in range(count - 1)])
    high = lax.ppermute(top, SP, [(i + 1, i) for i in range(count - 1)])
    long = group_rows + 2 * WINDOW_REACH
    attended = pl.pallas_call(
        attention_kernel,
        out_shape=shape_of(wide, BF16),
        in_specs=[SMEM] * 2 + [VMEM] * 5,
        out_specs=VMEM,
        scratch_shapes=[
            pltpu.VMEM((long, HEAD_DIM), BF16),
            pltpu.VMEM((long, 2 * HEAD_DIM), BF16),
            pltpu.VMEM((count * ctx_rows, 2 * HEAD_DIM), BF16),
        ],
        name="attention",
        compiler_params=vmem(16),
    )(where, sink_logit_head, *held(queries, low, pairs, high, ctx_pairs))
    attended = exchanged(attended.reshape(nx, nc * rows, 2 * HEAD_DIM), "x")
    weights = pl.pallas_call(
        load_kernel,
        out_shape=pltpu.VMEM((2, *out_weight.shape), BF16),
        in_specs=[HBM] * 2,
        out_specs=VMEM,
        scratch_shapes=[pltpu.SemaphoreType.DMA((2,))],
        name="load",
        compiler_params=vmem(2),
    )(*far(out_weight, out_others[0]))
    send, keep = pl.pallas_call(
        project_kernel,
        out_shape=[pltpu.VMEM((rows, width), BF16), pltpu.VMEM((rows, width), F32)],
        in_specs=[SMEM, VMEM, VMEM, HBM, HBM],
        out_specs=(VMEM, VMEM),
        scratch_shapes=[
            pltpu.VMEM((nc * rows, nx * 2 * HEAD_DIM), BF16),
            pltpu.VMEM((2, 2 * HEAD_DIM, width), BF16),
            pltpu.SemaphoreType.DMA((4, 2)),
        ],
        name="project",
        compiler_params=vmem(14),
    )(where, *held(attended, weights), *far(*out_others[1:]))
    got = swapped(send)
    return pl.pallas_call(
        final_kernel,
        out_shape=shape_of((rows, width), BF16),
        in_specs=[VMEM] * 4,
        out_specs=VMEM,
        name="final",
        compiler_params=vmem(8),
    )(*held(latent, keep, got, planes))


def solution(mesh):
    torus = Mesh(mesh.devices.reshape(16, 4, 4, 2), ALL)

    return jax.shard_map(
        shards,
        mesh=torus,
        in_specs=(
            P(ALL, None),
            P(SP),
            P(SP),
            P(SP, None),
            P(),
            P(SP, TP),
            P(SP, TP),
            P(SP, TP),
            P(None, TP),
            P(None, TP),
            P(None, TP),
            P(TP),
            P(TP, None),
        ),
        out_specs=P(ALL, None),
        check_vma=False,
    )
```
